512 devices in a mesh: fs: 64 (over z, y), tp: 8 (over x, core).
Axes of the slice: x: 4, y: 8, z: 8, core: 2. Of those that a mesh axis runs over, the one named last changes fastest.
Arguments:
- normed: bfloat16 [65536, 2048], P('fs'), may hold values from -6 to 6
- key_cot: bfloat16 [65536, 1024], P('fs', 'tp'), may hold values from -130 to 130
- value_cot: bfloat16 [65536, 2048], P('fs', 'tp'), may hold values from -130 to 130
- basis: bfloat16 [2048, 256], P('fs'), may hold values from -3.535534 to 3.535534
- master_key: float32 [2048, 1024], P('fs', 'tp'), may hold values from -3 to 3
- master_value: float32 [2048, 2048], P('fs', 'tp'), may hold values from -3 to 3
- first_key: float32 [256, 1024], P('fs', 'tp'), may hold values from -3 to 3
- second_key: float32 [256, 1024], P('fs', 'tp'), may hold values from 0.05 to 2
- first_value: float32 [256, 2048], P('fs', 'tp'), may hold values from -3 to 3
- second_value: float32 [256, 2048], P('fs', 'tp'), may hold values from 0.05 to 2
Outputs:
- step_key: float32 [2048, 1024], P('fs', 'tp')
- step_value: float32 [2048, 2048], P('fs', 'tp')
- new_master_key: float32 [2048, 1024], P('fs', 'tp')
- new_master_value: float32 [2048, 2048], P('fs', 'tp')
- copy_key: bfloat16 [2048, 1024], P(None, 'tp')
- copy_value: bfloat16 [2048, 2048], P(None, 'tp')
- new_first_key: float32 [256, 1024], P('fs', 'tp')
- new_second_key: float32 [256, 1024], P('fs', 'tp')
- new_first_value: float32 [256, 2048], P('fs', 'tp')
- new_second_value: float32 [256, 2048], P('fs', 'tp')
The draws below stay inside these ranges and needn't reach their ends.
All inputs are finite; a program needn't handle non-finite values.
Results may differ from the reference program's by a relative error of at most 0.0055.
Values may be sent and summed in bfloat16 or wider, within the bound.
A program may use at most 64 MiB of HBM per device.

```python
import math
import jax
import jax.numpy as jnp
from jax import lax

D = 2048
DK = 1024
DV = 2048
R = 256
TOKENS = 65536


def column_scaled(key, height, width):
    keys = jax.random.split(key, 2)
    ramp = jnp.arange(width, dtype=jnp.float32) / max(width - 1, 1)
    jitter = jnp.exp(jax.random.uniform(keys[1], (width,), jnp.float32, math.log(0.7), math.log(1.4)))
    scales = 10.0 ** ramp * jitter
    base_values = jnp.clip(jax.random.normal(keys[0], (height, width), jnp.float32), -6.0, 6.0)
    return base_values * scales[None, :]


def draw_basis(key, part):
    values = column_scaled(jax.random.fold_in(key, 11), D, R) * D ** (-0.5)
    return values.astype(jnp.bfloat16)


def draw_key_cot(key, part):
    return column_scaled(jax.random.fold_in(key, 12), TOKENS, DK).astype(jnp.bfloat16)


def draw_value_cot(key, part):
    return column_scaled(jax.random.fold_in(key, 13), TOKENS, DV).astype(jnp.bfloat16)


def shard_levels(stream_key, dims, cuts, low, largest):
    factor_of, own = 1.0, jax.random.fold_in(stream_key, 6)
    for dim, blocks in cuts:
        steps = jnp.exp(jax.random.uniform(jax.random.fold_in(own, dim), (blocks,), jnp.float32, low / len(cuts), largest / len(cuts)))
        factor_of = factor_of * jnp.repeat(steps, dims[dim] // blocks).reshape([-1 if axis == dim else 1 for axis in range(len(dims))])
    return factor_of


def noise(stream_key, extent, deviation, limit, cuts=(), kind=jnp.bfloat16):
    gain = shard_levels(stream_key, extent, cuts, -0.22, 0.18) if cuts else 1.0
    drawn = jax.random.normal(stream_key, extent, jnp.float32) * deviation * gain
    return jnp.minimum(jnp.maximum(drawn, -limit), limit).astype(kind)


def setup_inputs(seed: int = 0) -> dict:
    arg_keys = jax.random.split(jax.random.key(seed), 11)
    return {
        "normed": noise(arg_keys[0], (TOKENS, D), 1.0, 6.0, ((0, 64),)),
        "key_cot": draw_key_cot(jax.random.fold_in(arg_keys[10], 71), 0),
        "value_cot": draw_value_cot(jax.random.fold_in(arg_keys[10], 71), 0),
        "basis": draw_basis(jax.random.fold_in(arg_keys[10], 71), 0),
        "master_key": noise(arg_keys[4], (D, DK), 0.5, 3.0, ((0, 64), (1, 8)), jnp.float32),
        "master_value": noise(arg_keys[5], (D, DV), 0.5, 3.0, ((0, 64), (1, 8)), jnp.float32),
        "first_key": noise(arg_keys[6], (R, DK), 0.5, 3.0, ((0, 64), (1, 8)), jnp.float32),
        "second_key": jnp.clip(jnp.exp(math.log(2.0) - 3.6888794 * jax.random.uniform(arg_keys[7], (R, DK), jnp.float32) ** shard_levels(arg_keys[7], (R, DK), ((0, 64), (1, 8)), -0.2, 0.2)), 0.05, 2.0),
        "first_value": noise(arg_keys[8], (R, DV), 0.5, 3.0, ((0, 64), (1, 8)), jnp.float32),
        "second_value": jnp.clip(jnp.exp(math.log(2.0) - 3.6888794 * jax.random.uniform(arg_keys[9], (R, DV), jnp.float32) ** shard_levels(arg_keys[9], (R, DV), ((0, 64), (1, 8)), -0.2, 0.2)), 0.05, 2.0),
    }


learn_rate = 0.05
beta_first = 0.9
beta_second = 0.9
epsilon = 1e-08
norm_eps = 1e-06

def moment_update(low_grad, grad_scale, first_moment, second_moment, basis):
    scaled = low_grad * grad_scale
    new_first = beta_first * first_moment + (1.0 - beta_first) * scaled
    new_second = beta_second * second_moment + (1.0 - beta_second) * scaled * scaled
    direction = (new_first / (jnp.sqrt(new_second) + epsilon)).astype(jnp.bfloat16)
    update_step = jnp.dot(basis, direction, preferred_element_type=jnp.float32)
    return (update_step, new_first, new_second)

def reference(normed, key_cot, value_cot, basis, master_key, master_value, first_key, second_key, first_value, second_value):
    grad_key = jnp.dot(normed.T, key_cot, preferred_element_type=jnp.float32)
    grad_value = jnp.dot(normed.T, value_cot, preferred_element_type=jnp.float32)
    basis_wide = basis.astype(jnp.float32).T
    low_key = jnp.dot(basis_wide, grad_key, precision=lax.Precision.HIGHEST, preferred_element_type=jnp.float32)
    low_value = jnp.dot(basis_wide, grad_value, precision=lax.Precision.HIGHEST, preferred_element_type=jnp.float32)
    squares = jnp.sum(low_key * low_key) + jnp.sum(low_value * low_value)
    root_mean = jnp.sqrt(squares / (R * (DK + DV)) + norm_eps)
    grad_scale = 1.0 / root_mean
    step_key, new_first_key, new_second_key = moment_update(low_key, grad_scale, first_key, second_key, basis)
    step_value, new_first_value, new_second_value = moment_update(low_value, grad_scale, first_value, second_value, basis)
    new_master_key = master_key - learn_rate * step_key
    new_master_value = master_value - learn_rate * step_value
    return (step_key, step_value, new_master_key, new_master_value, new_master_key.astype(jnp.bfloat16), new_master_value.astype(jnp.bfloat16), new_first_key, new_second_key, new_first_value, new_second_value)
```

```python
import functools

import jax
import jax.numpy as jnp
from jax import lax
from jax.experimental import pallas as pl
from jax.experimental.pallas import tpu as pltpu
from jax.sharding import PartitionSpec as P

learn_rate = 0.05
beta_first = 0.9
beta_second = 0.9
epsilon = 1e-08
norm_eps = 1e-06

MESH = pl.DeviceIdType.MESH
F32 = jnp.float32
BF16 = jnp.bfloat16
SIDE = 8
NEAR = (1, 7, 2, 6, 3, 5, 4)
FAR = (4, 3, 5, 2, 6, 1, 7)


def distance(k):
    return min(k, SIDE - k)


def wait_recv(ref, sem):
    pltpu.make_async_remote_copy(
        src_ref=ref, dst_ref=ref, send_sem=sem, recv_sem=sem, device_id={"fs": 0}, device_id_type=MESH
    ).wait_recv()


def wait_send(ref, sem):
    pltpu.make_async_remote_copy(
        src_ref=ref, dst_ref=ref, send_sem=sem, recv_sem=sem, device_id={"fs": 0}, device_id_type=MESH
    ).wait_send()


def send(ref, target_ref, send_sem, recv_sem, **device):
    pltpu.make_async_remote_copy(
        src_ref=ref,
        dst_ref=target_ref,
        send_sem=send_sem,
        recv_sem=recv_sem,
        device_id=device,
        device_id_type=MESH,
    ).start()


def exchange_kernel(
    n,
    tp,
    count,
    normed,
    key_cot,
    value_cot,
    basis_in,
    master_key,
    master_value,
    first_key_in,
    second_key_in,
    first_value_in,
    second_value_in,
    basis_all,
    master_all,
    dirs,
    scaled_out,
    normed_v,
    key_v,
    value_v,
    master_key_v,
    master_value_v,
    first_key,
    second_key,
    first_value,
    second_value,
    moments,
    cot_t,
    grad_t,
    partial,
    received,
    low_own,
    low_all,
    turned,
    chip_own,
    chip_all,
    square_own,
    square_all,
    load_sem,
    basis_send,
    basis_one,
    basis_two,
    core_send,
    core_one,
    core_two,
    pack_send,
    pack_one,
    pack_near,
    part_send,
    part_recv,
    low_send,
    low_recv,
    chip_send,
    chip_recv,
    square_send,
    square_recv,
):
    me = lax.axis_index("fs")
    my_tp = lax.axis_index("tp")
    z, y = me // SIDE, lax.rem(me, SIDE)
    core = lax.rem(my_tp, 2)
    partner = my_tp + 1 - 2 * core

    def along(part, k):
        if part == 0:
            return lax.rem(z + k, SIDE) * SIDE + y
        return z * SIDE + lax.rem(y + k, SIDE)

    rows = basis_in.shape[0]
    half = rows // 2
    kc = key_cot.shape[1]

    loads = [
        pltpu.make_async_copy(source, target, load_sem.at[i])
        for i, (source, target) in enumerate(
            (
                (basis_in.at[:, 0:128], basis_all.at[0, z, y]),
                (basis_in.at[:, 128:256], basis_all.at[1, z, y]),
                (master_key, master_key_v),
                (master_value, master_value_v),
                (first_key_in, first_key),
                (second_key_in, second_key),
                (first_value_in, first_value),
                (second_value_in, second_value),
                (key_cot, key_v),
                (value_cot, value_v),
                (normed, normed_v),
            )
        )
    ]
    for load in loads:
        load.start()

    barrier = pltpu.get_barrier_semaphore()
    for k in range(1, SIDE):
        pl.semaphore_signal(barrier, inc=1, device_id={"fs": along(0, k)}, device_id_type=MESH)
        pl.semaphore_signal(barrier, inc=1, device_id={"fs": along(1, k)}, device_id_type=MESH)
    for k in range(1, tp):
        pl.semaphore_signal(barrier, inc=1, device_id={"tp": lax.rem(my_tp + k, tp)}, device_id_type=MESH)

    for load in loads[2:8]:
        load.wait()
    master_all[z, y, :, :kc] = master_key_v[...].astype(BF16)
    master_all[z, y, :, kc:] = master_value_v[...].astype(BF16)
    moments[0, z, y, :, :kc] = first_key[...].astype(BF16)
    moments[0, z, y, :, kc:] = first_value[...].astype(BF16)
    moments[1, z, y, :, :kc] = second_key[...].astype(BF16)
    moments[1, z, y, :, kc:] = second_value[...].astype(BF16)
    loads[0].wait()
    loads[1].wait()

    pl.semaphore_wait(barrier, 2 * (SIDE - 1) + tp - 1)

    spans = (pl.ds(0, half), pl.ds(half, half))

    def basis_at(part, zz, yy):
        return basis_all.at[core, zz, yy, spans[part], :]

    def basis_group(part, k):
        if part == 0:
            return basis_all.at[core, :, lax.rem(y + k, SIDE), spans[0], :]
        return basis_all.at[core, lax.rem(z + k, SIDE), :, spans[1], :]

    def other_group(part, k):
        if part == 0:
            return basis_all.at[1 - core, :, lax.rem(y + k, SIDE), spans[0], :]
        return basis_all.at[1 - core, lax.rem(z + k, SIDE), :, spans[1], :]

    def line_at(part, k):
        if part == 0:
            return lax.rem(z + k, SIDE), y
        return z, lax.rem(y + k, SIDE)

    for k in FAR:
        for part in range(2):
            own = basis_at(part, z, y)
            send(own, own, basis_send.at[part], basis_one.at[part, k], fs=along(part, k))

    for j in (0,) + NEAR:
        for part in range(2):
            block = basis_at(part, *line_at(part, SIDE - j))
            if j:
                wait_recv(block, basis_one.at[part, j])
            for k in FAR:
                send(block, block, basis_send.at[2 + part], basis_two.at[part, k], fs=along(1 - part, k))
            if j:
                send(block, block, core_send.at[part], core_one.at[part, j], tp=partner)

    def pack_at(part, zz, yy):
        return master_all.at[zz, yy, spans[part], :], moments.at[part, zz, yy]

    def pack_group(part, k, cut=slice(None)):
        cut = pl.ds(cut.start, cut.stop - cut.start) if cut.start is not None else slice(None)
        if part == 0:
            at = lax.rem(y + k, SIDE)
            return master_all.at[cut, at, spans[0], :], moments.at[0, cut, at]
        at = lax.rem(z + k, SIDE)
        return master_all.at[at, cut, spans[1], :], moments.at[1, at, cut]

    for k in FAR:
        for part in range(2):
            for a, block in enumerate(pack_at(part, z, y)):
                send(block, block, pack_send.at[part, a], pack_one.at[part, a, k], fs=along(part, k))

    loads[8].wait()
    loads[9].wait()
    cot_t[:kc, :] = key_v[...].T
    cot_t[kc:, :] = value_v[...].T
    loads[10].wait()
    tile = 256

    @pl.loop(0, normed_v.shape[1] // tile)
    def _(t):
        at = pl.ds(pl.multiple_of(t * tile, tile), tile)
        grad_t[:, at] = jnp.dot(cot_t[...], normed_v[:, at], preferred_element_type=F32).astype(BF16)

    for k in NEAR:
        for part in range(2):
            group = basis_group(part, SIDE - k)
            wait_recv(group, basis_two.at[part, k])
            send(group, group, core_send.at[2 + part], core_two.at[part, k], tp=partner)
    for k in NEAR:
        for part in range(2):
            zz, yy = line_at(part, SIDE - k)
            wait_recv(basis_all.at[1 - core, zz, yy, spans[part], :], core_one.at[part, k])
            wait_recv(other_group(part, SIDE - k), core_two.at[part, k])

    depth = n * rows
    whole = jnp.concatenate(
        [basis_all[0].reshape(depth, 128), basis_all[1].reshape(depth, 128)], axis=1
    )
    sums = jnp.dot(grad_t[...], whole, preferred_element_type=F32).T.astype(BF16)
    rank_rows = first_key.shape[0]
    for j in range(n):
        partial[j] = sums[j * rank_rows : (j + 1) * rank_rows, :]

    order = sorted(
        ((dz, dy) for dz in range(SIDE) for dy in range(SIDE) if dz or dy),
        key=lambda d: -distance(d[0]) - distance(d[1]),
    )

    def device(dz, dy):
        return lax.rem(z + dz, SIDE) * SIDE + lax.rem(y + dy, SIDE)

    for dz, dy in order:
        target = device(dz, dy)
        send(partial.at[target], received.at[dz * SIDE + dy], part_send.at[0], part_recv.at[0], fs=target)

    for k in NEAR:
        for part in range(2):
            for a, block in enumerate(pack_at(part, *line_at(part, SIDE - k))):
                wait_recv(block, pack_one.at[part, a, k])
    for k in (2, 6, 1, 7):
        for part in range(2):
            for a, group in enumerate(pack_group(part, 0)):
                send(group, group, pack_send.at[2 + part, a], pack_near.at[part, a, k], fs=along(1 - part, k))

    wait_recv(received.at[pl.ds(1, n - 1)], part_recv.at[0])
    low = partial[me].astype(F32)
    for k in range(1, n):
        low = low + received[k].astype(F32)

    chip_own[...] = jnp.full(chip_own.shape, jnp.sum(low * low), F32)
    low_own[...] = low.astype(BF16)
    low_all[me] = low.astype(BF16)
    for k in range(1, tp):
        send(chip_own, chip_all.at[k], chip_send.at[0], chip_recv.at[0], tp=lax.rem(my_tp + k, tp))
    for dz, dy in order:
        send(low_own, low_all.at[me], low_send.at[0], low_recv.at[0], fs=device(dz, dy))
    wait_recv(chip_all.at[pl.ds(1, tp - 1)], chip_recv.at[0])
    square = chip_own[...] + jnp.sum(chip_all[1:], axis=0)
    square_own[...] = square
    for dz, dy in order:
        send(square_own, square_all.at[dz * SIDE + dy], square_send.at[0], square_recv.at[0], fs=device(dz, dy))

    for k, ahead, cut in ((2, 1, slice(0, SIDE // 2)), (6, 7, slice(SIDE // 2, SIDE))):
        for part in range(2):
            for a, group in enumerate(pack_group(part, SIDE - k)):
                wait_recv(group, pack_near.at[part, a, k])
                send(
                    group,
                    group,
                    pack_send.at[4 + part, a],
                    pack_near.at[part, a, (k + ahead) % SIDE],
                    fs=along(1 - part, ahead),
                )
            for a, group in enumerate(pack_group(part, SIDE - k, cut)):
                send(
                    group, group, pack_send.at[6 + part, a], pack_near.at[part, a, 0 if k == 2 else 4], fs=along(1 - part, k)
                )

    wait_recv(square_all.at[pl.ds(1, n - 1)], square_recv.at[0])
    total = square_own[...] + jnp.sum(square_all[1:], axis=0)
    grad_scale = (1.0 / jnp.sqrt(total / count + norm_eps))[0:1, 0:1]
    scaled_out[...] = low * grad_scale

    for k in (1, 7, 3, 5):
        for part in range(2):
            for a, group in enumerate(pack_group(part, SIDE - k)):
                wait_recv(group, pack_near.at[part, a, k])
    for slot, cut in ((0, slice(0, SIDE // 2)), (4, slice(SIDE // 2, SIDE))):
        for part in range(2):
            for a, group in enumerate(pack_group(part, SIDE // 2, cut)):
                wait_recv(group, pack_near.at[part, a, slot])
    wait_recv(low_all.at[pl.ds(0, n - 1)], low_recv.at[0])

    for j in range(n):
        scaled = low_all[j].astype(F32) * grad_scale
        moved = beta_first * moments[0, j // SIDE, j % SIDE].astype(F32) + (1.0 - beta_first) * scaled
        spread = beta_second * moments[1, j // SIDE, j % SIDE].astype(F32) + (1.0 - beta_second) * scaled * scaled
        turned[j * rank_rows : (j + 1) * rank_rows, :] = moved / (jnp.sqrt(spread) + epsilon)
    dirs[...] = turned[...].astype(BF16)

    own_line = basis_all.at[0, pl.ds(0, SIDE - 1), 0, spans[0], :]
    for part in range(2):
        wait_send(own_line, basis_send.at[part])
        wait_send(own_line, core_send.at[part])
        wait_send(basis_all.at[0, :, pl.ds(0, SIDE - 1), spans[0], :], basis_send.at[2 + part])
        wait_send(basis_all.at[0, :, pl.ds(0, SIDE - 1), spans[0], :], core_send.at[2 + part])
        for a, array in enumerate((lambda *at: master_all.at[(*at, spans[0])], lambda *at: moments.at[(0, *at)])):
            wait_send(array(pl.ds(0, SIDE - 1), 0), pack_send.at[part, a])
            wait_send(array(slice(None), pl.ds(0, 4)), pack_send.at[2 + part, a])
            wait_send(array(slice(None), pl.ds(0, 2)), pack_send.at[4 + part, a])
            wait_send(array(slice(None), 0), pack_send.at[6 + part, a])
    wait_send(partial.at[pl.ds(0, n - 1)], part_send.at[0])
    wait_send(low_all.at[pl.ds(0, n - 1)], low_send.at[0])
    wait_send(chip_all.at[pl.ds(1, tp - 1)], chip_send.at[0])
    wait_send(square_all.at[pl.ds(1, n - 1)], square_send.at[0])


def final_kernel(
    basis_all,
    master_all,
    dirs,
    basis,
    master_key,
    master_value,
    scaled,
    first_key,
    second_key,
    first_value,
    second_value,
    copy_key,
    copy_value,
    step_key,
    step_value,
    new_key,
    new_value,
    new_first_key,
    new_second_key,
    new_first_value,
    new_second_value,
):
    kc = copy_key.shape[1]
    whole = jnp.concatenate([basis_all[0], basis_all[1]], axis=1)
    for cut, out in ((slice(0, kc), copy_key), (slice(kc, None), copy_value)):
        step = jnp.dot(whole, dirs[:, cut], preferred_element_type=F32)
        out[...] = (master_all[:, cut].astype(F32) - learn_rate * step).astype(BF16)

    @pl.when(pl.program_id(0) == 0)
    def _():
        for cut, master, step_out, new in (
            (slice(0, kc), master_key, step_key, new_key),
            (slice(kc, None), master_value, step_value, new_value),
        ):
            step = jnp.dot(basis[...], dirs[:, cut], preferred_element_type=F32)
            step_out[...] = step
            new[...] = master[...] - learn_rate * step
        for cut, first, second, new_first, new_second in (
            (slice(0, kc), first_key, second_key, new_first_key, new_second_key),
            (slice(kc, None), first_value, second_value, new_first_value, new_second_value),
        ):
            own = scaled[:, cut]
            new_first[...] = beta_first * first[...] + (1.0 - beta_first) * own
            new_second[...] = beta_second * second[...] + (1.0 - beta_second) * own * own


def on_device(
    n,
    tp,
    normed,
    key_cot,
    value_cot,
    basis,
    master_key,
    master_value,
    first_key,
    second_key,
    first_value,
    second_value,
):
    rows, rank = basis.shape
    d = rows * n
    kc, vc = key_cot.shape[1], value_cot.shape[1]
    cols = kc + vc
    tokens = normed.shape[0]
    rank_rows = first_key.shape[0]
    vmem = pl.BlockSpec(memory_space=pltpu.VMEM)
    hbm = pl.BlockSpec(memory_space=pl.ANY)
    dma = pltpu.SemaphoreType.DMA
    small = (1, 128)
    basis_all, master_all, dirs, scaled = pl.pallas_call(
        functools.partial(exchange_kernel, n, tp, rank * cols * tp),
        out_shape=(
            jax.ShapeDtypeStruct((2, SIDE, SIDE, rows, rank // 2), BF16),
            jax.ShapeDtypeStruct((SIDE, SIDE, rows, cols), BF16),
            jax.ShapeDtypeStruct((rank, cols), BF16),
            jax.ShapeDtypeStruct((rank_rows, cols), F32),
        ),
        in_specs=[hbm] * 10,
        out_specs=[vmem] * 4,
        scratch_shapes=[
            pltpu.VMEM(normed.shape, BF16),
            pltpu.VMEM(key_cot.shape, BF16),
            pltpu.VMEM(value_cot.shape, BF16),
            pltpu.VMEM(master_key.shape, F32),
            pltpu.VMEM(master_value.shape, F32),
            pltpu.VMEM(first_key.shape, F32),
            pltpu.VMEM(first_key.shape, F32),
            pltpu.VMEM(first_value.shape, F32),
            pltpu.VMEM(first_value.shape, F32),
            pltpu.VMEM((2, SIDE, SIDE, rank_rows, cols), BF16),
            pltpu.VMEM((cols, tokens), BF16),
            pltpu.VMEM((cols, d), BF16),
            pltpu.VMEM((n, rank_rows, cols), BF16),
            pltpu.VMEM((n, rank_rows, cols), BF16),
            pltpu.VMEM((rank_rows, cols), BF16),
            pltpu.VMEM((n, rank_rows, cols), BF16),
            pltpu.VMEM((rank, cols), F32),
            pltpu.VMEM(small, F32),
            pltpu.VMEM((tp, *small), F32),
            pltpu.VMEM(small, F32),
            pltpu.VMEM((n, *small), F32),
            dma((11,)),
            dma((4,)),
            dma((2, SIDE)),
            dma((2, SIDE)),
            dma((4,)),
            dma((2, SIDE)),
            dma((2, SIDE)),
            dma((8, 2)),
            dma((2, 2, SIDE)),
            dma((2, 2, SIDE)),
        ]
        + [dma((1,))] * 8,
        compiler_params=pltpu.CompilerParams(
            collective_id=0, has_side_effects=True, vmem_limit_bytes=67_043_328
        ),
    )(normed, key_cot, value_cot, basis, master_key, master_value, first_key, second_key, first_value, second_value)
    basis_all = basis_all.reshape(2, d, rank // 2)
    master_all = master_all.reshape(d, cols)

    block = d // 2
    whole = lambda *shape: pl.BlockSpec(shape, lambda i: (0,) * len(shape))
    sliced = lambda width: pl.BlockSpec((block, width), lambda i: (i, 0))
    moments = [whole(rank_rows, kc)] * 2 + [whole(rank_rows, vc)] * 2
    copy_key, copy_value, step_key, step_value, new_key, new_value, nfk, nsk, nfv, nsv = pl.pallas_call(
        final_kernel,
        grid=(d // block,),
        out_shape=(
            jax.ShapeDtypeStruct((d, kc), BF16),
            jax.ShapeDtypeStruct((d, vc), BF16),
            jax.ShapeDtypeStruct((rows, kc), F32),
            jax.ShapeDtypeStruct((rows, vc), F32),
            jax.ShapeDtypeStruct((rows, kc), F32),
            jax.ShapeDtypeStruct((rows, vc), F32),
            jax.ShapeDtypeStruct(first_key.shape, F32),
            jax.ShapeDtypeStruct(first_key.shape, F32),
            jax.ShapeDtypeStruct(first_value.shape, F32),
            jax.ShapeDtypeStruct(first_value.shape, F32),
        ),
        in_specs=[
            pl.BlockSpec((2, block, rank // 2), lambda i: (0, i, 0)),
            sliced(cols),
            whole(rank, cols),
            whole(rows, rank),
            whole(rows, kc),
            whole(rows, vc),
            whole(rank_rows, cols),
            *moments,
        ],
        out_specs=[sliced(kc), sliced(vc), whole(rows, kc), whole(rows, vc), whole(rows, kc), whole(rows, vc), *moments],
    )(
        basis_all, master_all, dirs, basis, master_key, master_value, scaled, first_key, second_key, first_value, second_value
    )
    return (step_key, step_value, new_key, new_value, copy_key, copy_value, nfk, nsk, nfv, nsv)


def solution(mesh):
    split = P("fs", "tp")
    lone = P("fs", None)
    return jax.shard_map(
        functools.partial(on_device, mesh.shape["fs"], mesh.shape["tp"]),
        mesh=mesh,
        in_specs=(lone, split, split, lone) + (split,) * 6,
        out_specs=(split,) * 4 + (P(None, "tp"),) * 2 + (split,) * 4,
        check_vma=False,
    )
```

```python
import functools

import jax
import jax.numpy as jnp
from jax import lax
from jax.experimental import pallas as pl
from jax.experimental.pallas import tpu as pltpu
from jax.sharding import PartitionSpec as P

learn_rate = 0.05
beta_first = 0.9
beta_second = 0.9
epsilon = 1e-08
norm_eps = 1e-06

MESH = pl.DeviceIdType.MESH
F32 = jnp.float32
BF16 = jnp.bfloat16
SIDE = 8
NEAR = (1, 7, 2, 6, 3, 5, 4)
FAR = (4, 3, 5, 2, 6, 1, 7)


def distance(k):
    return min(k, SIDE - k)


def wait_recv(ref, sem):
    pltpu.make_async_remote_copy(
        src_ref=ref, dst_ref=ref, send_sem=sem, recv_sem=sem, device_id={"fs": 0}, device_id_type=MESH
    ).wait_recv()


def wait_send(ref, sem):
    pltpu.make_async_remote_copy(
        src_ref=ref, dst_ref=ref, send_sem=sem, recv_sem=sem, device_id={"fs": 0}, device_id_type=MESH
    ).wait_send()


def send(ref, target_ref, send_sem, recv_sem, **device):
    pltpu.make_async_remote_copy(
        src_ref=ref,
        dst_ref=target_ref,
        send_sem=send_sem,
        recv_sem=recv_sem,
        device_id=device,
        device_id_type=MESH,
    ).start()


def exchange_kernel(
    n,
    tp,
    count,
    normed,
    key_cot,
    value_cot,
    basis_in,
    master_key,
    master_value,
    first_key_in,
    second_key_in,
    first_value_in,
    second_value_in,
    basis_all,
    master_all,
    dirs,
    scaled_out,
    normed_v,
    key_v,
    value_v,
    master_key_v,
    master_value_v,
    first_key,
    second_key,
    first_value,
    second_value,
    moments,
    cot_t,
    grad_t,
    partial,
    received,
    low_own,
    low_all,
    turned,
    chip_own,
    chip_all,
    square_own,
    square_all,
    load_sem,
    basis_send,
    basis_one,
    basis_two,
    core_send,
    core_one,
    core_two,
    pack_send,
    pack_one,
    pack_near,
    part_send,
    part_recv,
    low_send,
    low_recv,
    chip_send,
    chip_recv,
    square_send,
    square_recv,
):
    me = lax.axis_index("fs")
    my_tp = lax.axis_index("tp")
    z, y = me // SIDE, lax.rem(me, SIDE)
    core = lax.rem(my_tp, 2)
    partner = my_tp + 1 - 2 * core

    def along(part, k):
        if part == 0:
            return lax.rem(z + k, SIDE) * SIDE + y
        return z * SIDE + lax.rem(y + k, SIDE)

    rows = basis_in.shape[0]
    half = rows // 2
    kc = key_cot.shape[1]

    loads = [
        pltpu.make_async_copy(source, target, load_sem.at[i])
        for i, (source, target) in enumerate(
            (
                (basis_in.at[:, 0:128], basis_all.at[0, z, y]),
                (basis_in.at[:, 128:256], basis_all.at[1, z, y]),
                (master_key, master_key_v),
                (master_value, master_value_v),
                (first_key_in, first_key),
                (second_key_in, second_key),
                (first_value_in, first_value),
                (second_value_in, second_value),
                (key_cot, key_v),
                (value_cot, value_v),
                (normed, normed_v),
            )
        )
    ]
    barrier = pltpu.get_barrier_semaphore()
    for k in range(1, SIDE):
        pl.semaphore_signal(barrier, inc=1, device_id={"fs": along(0, k)}, device_id_type=MESH)
        pl.semaphore_signal(barrier, inc=1, device_id={"fs": along(1, k)}, device_id_type=MESH)
    for k in range(1, tp):
        pl.semaphore_signal(barrier, inc=1, device_id={"tp": lax.rem(my_tp + k, tp)}, device_id_type=MESH)

    for load in loads:
        load.start()

    loads[0].wait()
    loads[1].wait()
    pl.semaphore_wait(barrier, 2 * (SIDE - 1) + tp - 1)

    spans = (pl.ds(0, half), pl.ds(half, half))

    def basis_at(part, zz, yy):
        return basis_all.at[core, zz, yy, spans[part], :]

    def basis_group(part, k):
        if part == 0:
            return basis_all.at[core, :, lax.rem(y + k, SIDE), spans[0], :]
        return basis_all.at[core, lax.rem(z + k, SIDE), :, spans[1], :]

    def other_group(part, k):
        if part == 0:
            return basis_all.at[1 - core, :, lax.rem(y + k, SIDE), spans[0], :]
        return basis_all.at[1 - core, lax.rem(z + k, SIDE), :, spans[1], :]

    def line_at(part, k):
        if part == 0:
            return lax.rem(z + k, SIDE), y
        return z, lax.rem(y + k, SIDE)

    for k in FAR:
        for part in range(2):
            own = basis_at(part, z, y)
            send(own, own, basis_send.at[part], basis_one.at[part, k], fs=along(part, k))

    for j in (0,) + NEAR:
        for part in range(2):
            block = basis_at(part, *line_at(part, SIDE - j))
            if j:
                wait_recv(block, basis_one.at[part, j])
            for k in FAR:
                send(block, block, basis_send.at[2 + part], basis_two.at[part, k], fs=along(1 - part, k))
            if j:
                send(block, block, core_send.at[part], core_one.at[part, j], tp=partner)

    def pack_at(part, zz, yy):
        return master_all.at[zz, yy, spans[part], :], moments.at[part, zz, yy]

    def pack_group(part, k, cut=slice(None)):
        cut = pl.ds(cut.start, cut.stop - cut.start) if cut.start is not None else slice(None)
        if part == 0:
            at = lax.rem(y + k, SIDE)
            return master_all.at[cut, at, spans[0], :], moments.at[0, cut, at]
        at = lax.rem(z + k, SIDE)
        return master_all.at[at, cut, spans[1], :], moments.at[1, at, cut]

    for load in loads[2:8]:
        load.wait()
    master_all[z, y, :, :kc] = master_key_v[...].astype(BF16)
    master_all[z, y, :, kc:] = master_value_v[...].astype(BF16)
    moments[0, z, y, :, :kc] = first_key[...].astype(BF16)
    moments[0, z, y, :, kc:] = first_value[...].astype(BF16)
    moments[1, z, y, :, :kc] = second_key[...].astype(BF16)
    moments[1, z, y, :, kc:] = second_value[...].astype(BF16)

    for k in FAR:
        for part in range(2):
            for a, block in enumerate(pack_at(part, z, y)):
                send(block, block, pack_send.at[part, a], pack_one.at[part, a, k], fs=along(part, k))

    def pack_first():
        for k in NEAR:
            for part in range(2):
                for a, block in enumerate(pack_at(part, *line_at(part, SIDE - k))):
                    wait_recv(block, pack_one.at[part, a, k])
        for k in (1, 7):
            for part in range(2):
                for a, group in enumerate(pack_group(part, 0)):
                    send(group, group, pack_send.at[2 + part, a], pack_near.at[part, a, k], fs=along(1 - part, k))

    def pack_step(k):
        ahead = 1 if k < SIDE // 2 else SIDE - 1
        for part in range(2):
            for a, group in enumerate(pack_group(part, SIDE - k)):
                wait_recv(group, pack_near.at[part, a, k])
                send(
                    group,
                    group,
                    pack_send.at[4 + part, a],
                    pack_near.at[part, a, (k + ahead) % SIDE],
                    fs=along(1 - part, ahead),
                )
        if distance(k) == 2:
            cut = slice(0, SIDE // 2) if k == 2 else slice(SIDE // 2, SIDE)
            for part in range(2):
                for a, group in enumerate(pack_group(part, SIDE - k, cut)):
                    send(
                        group,
                        group,
                        pack_send.at[6 + part, a],
                        pack_near.at[part, a, 0 if k == 2 else 4],
                        fs=along(1 - part, k),
                    )

    loads[8].wait()
    loads[9].wait()
    cot_t[:kc, :] = key_v[...].T
    cot_t[kc:, :] = value_v[...].T
    loads[10].wait()
    tile = 256

    @pl.loop(0, normed_v.shape[1] // tile)
    def _(t):
        at = pl.ds(pl.multiple_of(t * tile, tile), tile)
        grad_t[:, at] = jnp.dot(cot_t[...], normed_v[:, at], preferred_element_type=F32).astype(BF16)

    pack_first()
    for k in NEAR:
        for part in range(2):
            group = basis_group(part, SIDE - k)
            wait_recv(group, basis_two.at[part, k])
            send(group, group, core_send.at[2 + part], core_two.at[part, k], tp=partner)
    for k in NEAR:
        for part in range(2):
            zz, yy = line_at(part, SIDE - k)
            wait_recv(basis_all.at[1 - core, zz, yy, spans[part], :], core_one.at[part, k])
            wait_recv(other_group(part, SIDE - k), core_two.at[part, k])

    depth = n * rows
    whole = jnp.concatenate(
        [basis_all[0].reshape(depth, 128), basis_all[1].reshape(depth, 128)], axis=1
    )
    sums = jnp.dot(grad_t[...], whole, preferred_element_type=F32).T.astype(BF16)
    rank_rows = first_key.shape[0]
    for j in range(n):
        partial[j] = sums[j * rank_rows : (j + 1) * rank_rows, :]

    order = sorted(
        ((dz, dy) for dz in range(SIDE) for dy in range(SIDE) if dz or dy),
        key=lambda d: -distance(d[0]) - distance(d[1]),
    )

    def device(dz, dy):
        return lax.rem(z + dz, SIDE) * SIDE + lax.rem(y + dy, SIDE)

    for dz, dy in order:
        target = device(dz, dy)
        send(partial.at[target], received.at[dz * SIDE + dy], part_send.at[0], part_recv.at[0], fs=target)

    pack_step(1)
    pack_step(7)

    wait_recv(received.at[pl.ds(1, n - 1)], part_recv.at[0])
    low = partial[me].astype(F32)
    for k in range(1, n):
        low = low + received[k].astype(F32)

    chip_own[...] = jnp.full(chip_own.shape, jnp.sum(low * low), F32)
    low_own[...] = low.astype(BF16)
    low_all[me] = low.astype(BF16)
    for k in range(1, tp):
        send(chip_own, chip_all.at[k], chip_send.at[0], chip_recv.at[0], tp=lax.rem(my_tp + k, tp))
    for dz, dy in order:
        send(low_own, low_all.at[me], low_send.at[0], low_recv.at[0], fs=device(dz, dy))
    wait_recv(chip_all.at[pl.ds(1, tp - 1)], chip_recv.at[0])
    square = chip_own[...] + jnp.sum(chip_all[1:], axis=0)
    square_own[...] = square
    for dz, dy in order:
        send(square_own, square_all.at[dz * SIDE + dy], square_send.at[0], square_recv.at[0], fs=device(dz, dy))

    pack_step(2)
    pack_step(6)

    wait_recv(square_all.at[pl.ds(1, n - 1)], square_recv.at[0])
    total = square_own[...] + jnp.sum(square_all[1:], axis=0)
    grad_scale = (1.0 / jnp.sqrt(total / count + norm_eps))[0:1, 0:1]
    scaled_out[...] = low * grad_scale

    for k in (3, 5):
        for part in range(2):
            for a, group in enumerate(pack_group(part, SIDE - k)):
                wait_recv(group, pack_near.at[part, a, k])
    for slot, cut in ((0, slice(0, SIDE // 2)), (4, slice(SIDE // 2, SIDE))):
        for part in range(2):
            for a, group in enumerate(pack_group(part, SIDE // 2, cut)):
                wait_recv(group, pack_near.at[part, a, slot])
    wait_recv(low_all.at[pl.ds(0, n - 1)], low_recv.at[0])

    for j in range(n):
        scaled = low_all[j].astype(F32) * grad_scale
        moved = beta_first * moments[0, j // SIDE, j % SIDE].astype(F32) + (1.0 - beta_first) * scaled
        spread = beta_second * moments[1, j // SIDE, j % SIDE].astype(F32) + (1.0 - beta_second) * scaled * scaled
        turned[j * rank_rows : (j + 1) * rank_rows, :] = moved / (jnp.sqrt(spread) + epsilon)
    dirs[...] = turned[...].astype(BF16)

    own_line = basis_all.at[0, pl.ds(0, SIDE - 1), 0, spans[0], :]
    for part in range(2):
        wait_send(own_line, basis_send.at[part])
        wait_send(own_line, core_send.at[part])
        wait_send(basis_all.at[0, :, pl.ds(0, SIDE - 1), spans[0], :], basis_send.at[2 + part])
        wait_send(basis_all.at[0, :, pl.ds(0, SIDE - 1), spans[0], :], core_send.at[2 + part])
        for a, array in enumerate((lambda *at: master_all.at[(*at, spans[0])], lambda *at: moments.at[(0, *at)])):
            wait_send(array(pl.ds(0, SIDE - 1), 0), pack_send.at[part, a])
            wait_send(array(slice(None), pl.ds(0, 2)), pack_send.at[2 + part, a])
            wait_send(array(slice(None), pl.ds(0, 4)), pack_send.at[4 + part, a])
            wait_send(array(slice(None), 0), pack_send.at[6 + part, a])
    wait_send(partial.at[pl.ds(0, n - 1)], part_send.at[0])
    wait_send(low_all.at[pl.ds(0, n - 1)], low_send.at[0])
    wait_send(chip_all.at[pl.ds(1, tp - 1)], chip_send.at[0])
    wait_send(square_all.at[pl.ds(1, n - 1)], square_send.at[0])


def final_kernel(
    basis_all,
    master_all,
    dirs,
    basis,
    master_key,
    master_value,
    scaled,
    first_key,
    second_key,
    first_value,
    second_value,
    copy_key,
    copy_value,
    step_key,
    step_value,
    new_key,
    new_value,
    new_first_key,
    new_second_key,
    new_first_value,
    new_second_value,
):
    kc = copy_key.shape[1]
    depth = copy_key.shape[0]
    block = depth // SIDE
    for i in range(SIDE):
        at = slice(i * block, (i + 1) * block)
        whole = jnp.concatenate([basis_all[h, i].reshape(block, 128) for h in range(2)], axis=1)
        held = master_all[i].reshape(block, dirs.shape[1])
        for cut, out in ((slice(0, kc), copy_key), (slice(kc, None), copy_value)):
            step = jnp.dot(whole, dirs[:, cut], preferred_element_type=F32)
            out[at, :] = (held[:, cut].astype(F32) - learn_rate * step).astype(BF16)

    for cut, master, step_out, new in (
        (slice(0, kc), master_key, step_key, new_key),
        (slice(kc, None), master_value, step_value, new_value),
    ):
        step = jnp.dot(basis[...], dirs[:, cut], preferred_element_type=F32)
        step_out[...] = step
        new[...] = master[...] - learn_rate * step
    for cut, first, second, new_first, new_second in (
        (slice(0, kc), first_key, second_key, new_first_key, new_second_key),
        (slice(kc, None), first_value, second_value, new_first_value, new_second_value),
    ):
        own = scaled[:, cut]
        new_first[...] = beta_first * first[...] + (1.0 - beta_first) * own
        new_second[...] = beta_second * second[...] + (1.0 - beta_second) * own * own


def on_device(
    n,
    tp,
    normed,
    key_cot,
    value_cot,
    basis,
    master_key,
    master_value,
    first_key,
    second_key,
    first_value,
    second_value,
):
    rows, rank = basis.shape
    d = rows * n
    kc, vc = key_cot.shape[1], value_cot.shape[1]
    cols = kc + vc
    tokens = normed.shape[0]
    rank_rows = first_key.shape[0]
    vmem = pl.BlockSpec(memory_space=pltpu.VMEM)
    hbm = pl.BlockSpec(memory_space=pltpu.HBM)
    dma = pltpu.SemaphoreType.DMA
    small = (1, 128)
    basis_all, master_all, dirs, scaled = pl.pallas_call(
        functools.partial(exchange_kernel, n, tp, rank * cols * tp),
        out_shape=(
            pltpu.VMEM((2, SIDE, SIDE, rows, rank // 2), BF16),
            pltpu.VMEM((SIDE, SIDE, rows, cols), BF16),
            pltpu.VMEM((rank, cols), BF16),
            pltpu.VMEM((rank_rows, cols), F32),
        ),
        in_specs=[hbm] * 10,
        out_specs=[vmem] * 4,
        scratch_shapes=[
            pltpu.VMEM(normed.shape, BF16),
            pltpu.VMEM(key_cot.shape, BF16),
            pltpu.VMEM(value_cot.shape, BF16),
            pltpu.VMEM(master_key.shape, F32),
            pltpu.VMEM(master_value.shape, F32),
            pltpu.VMEM(first_key.shape, F32),
            pltpu.VMEM(first_key.shape, F32),
            pltpu.VMEM(first_value.shape, F32),
            pltpu.VMEM(first_value.shape, F32),
            pltpu.VMEM((2, SIDE, SIDE, rank_rows, cols), BF16),
            pltpu.VMEM((cols, tokens), BF16),
            pltpu.VMEM((cols, d), BF16),
            pltpu.VMEM((n, rank_rows, cols), BF16),
            pltpu.VMEM((n, rank_rows, cols), BF16),
            pltpu.VMEM((rank_rows, cols), BF16),
            pltpu.VMEM((n, rank_rows, cols), BF16),
            pltpu.VMEM((rank, cols), F32),
            pltpu.VMEM(small, F32),
            pltpu.VMEM((tp, *small), F32),
            pltpu.VMEM(small, F32),
            pltpu.VMEM((n, *small), F32),
            dma((11,)),
            dma((4,)),
            dma((2, SIDE)),
            dma((2, SIDE)),
            dma((4,)),
            dma((2, SIDE)),
            dma((2, SIDE)),
            dma((8, 2)),
            dma((2, 2, SIDE)),
            dma((2, 2, SIDE)),
        ]
        + [dma((1,))] * 8,
        compiler_params=pltpu.CompilerParams(
            collective_id=0, has_side_effects=True, vmem_limit_bytes=62_914_560
        ),
    )(normed, key_cot, value_cot, basis, master_key, master_value, first_key, second_key, first_value, second_value)
    copy_key, copy_value, step_key, step_value, new_key, new_value, nfk, nsk, nfv, nsv = pl.pallas_call(
        final_kernel,
        out_shape=(
            jax.ShapeDtypeStruct((d, kc), BF16),
            jax.ShapeDtypeStruct((d, vc), BF16),
            jax.ShapeDtypeStruct((rows, kc), F32),
            jax.ShapeDtypeStruct((rows, vc), F32),
            jax.ShapeDtypeStruct((rows, kc), F32),
            jax.ShapeDtypeStruct((rows, vc), F32),
            jax.ShapeDtypeStruct(first_key.shape, F32),
            jax.ShapeDtypeStruct(first_key.shape, F32),
            jax.ShapeDtypeStruct(first_value.shape, F32),
            jax.ShapeDtypeStruct(first_value.shape, F32),
        ),
        in_specs=[vmem] * 11,
        out_specs=[vmem] * 10,
        compiler_params=pltpu.CompilerParams(vmem_limit_bytes=24 << 20),
    )(
        basis_all, master_all, dirs, basis, master_key, master_value, scaled, first_key, second_key, first_value, second_value
    )
    return (step_key, step_value, new_key, new_value, copy_key, copy_value, nfk, nsk, nfv, nsv)


def solution(mesh):
    split = P("fs", "tp")
    lone = P("fs", None)
    return jax.shard_map(
        functools.partial(on_device, mesh.shape["fs"], mesh.shape["tp"]),
        mesh=mesh,
        in_specs=(lone, split, split, lone) + (split,) * 6,
        out_specs=(split,) * 4 + (P(None, "tp"),) * 2 + (split,) * 4,
        check_vma=False,
    )
```

```python
import functools

import jax
import jax.numpy as jnp
from jax import lax
from jax.experimental import pallas as pl
from jax.experimental.pallas import tpu as pltpu
from jax.sharding import PartitionSpec as P

learn_rate = 0.05
beta_first = 0.9
beta_second = 0.9
epsilon = 1e-08
norm_eps = 1e-06

MESH = pl.DeviceIdType.MESH
F32 = jnp.float32
BF16 = jnp.bfloat16
SIDE = 8
NEAR = (1, 7, 2, 6, 3, 5, 4)
FAR = (4, 3, 5, 2, 6, 1, 7)


def distance(k):
    return min(k, SIDE - k)


def wait_recv(ref, sem):
    pltpu.make_async_remote_copy(
        src_ref=ref, dst_ref=ref, send_sem=sem, recv_sem=sem, device_id={"fs": 0}, device_id_type=MESH
    ).wait_recv()


def wait_send(ref, sem):
    pltpu.make_async_remote_copy(
        src_ref=ref, dst_ref=ref, send_sem=sem, recv_sem=sem, device_id={"fs": 0}, device_id_type=MESH
    ).wait_send()


def send(ref, target_ref, send_sem, recv_sem, **device):
    pltpu.make_async_remote_copy(
        src_ref=ref,
        dst_ref=target_ref,
        send_sem=send_sem,
        recv_sem=recv_sem,
        device_id=device,
        device_id_type=MESH,
    ).start()


def exchange_kernel(
    n,
    tp,
    count,
    normed,
    key_cot,
    value_cot,
    basis_in,
    master_key,
    master_value,
    first_key_in,
    second_key_in,
    first_value_in,
    second_value_in,
    basis_all,
    master_all,
    dirs,
    scaled_out,
    normed_v,
    key_v,
    value_v,
    master_key_v,
    master_value_v,
    first_key,
    second_key,
    first_value,
    second_value,
    moments,
    cot_t,
    grad_t,
    partial,
    received,
    low_own,
    low_all,
    turned,
    chip_own,
    chip_all,
    square_own,
    square_all,
    load_sem,
    basis_send,
    basis_one,
    basis_two,
    core_send,
    core_one,
    core_two,
    pack_send,
    pack_one,
    pack_near,
    part_send,
    part_recv,
    low_send,
    low_recv,
    chip_send,
    chip_recv,
    square_send,
    square_recv,
):
    me = lax.axis_index("fs")
    my_tp = lax.axis_index("tp")
    z, y = me // SIDE, lax.rem(me, SIDE)
    core = lax.rem(my_tp, 2)
    partner = my_tp + 1 - 2 * core

    def along(part, k):
        if part == 0:
            return lax.rem(z + k, SIDE) * SIDE + y
        return z * SIDE + lax.rem(y + k, SIDE)

    rows = basis_in.shape[0]
    kc = key_cot.shape[1]

    loads = [
        pltpu.make_async_copy(source, target, load_sem.at[i])
        for i, (source, target) in enumerate(
            (
                (basis_in.at[:, 0:128], basis_all.at[0, z, y]),
                (basis_in.at[:, 128:256], basis_all.at[1, z, y]),
                (master_key, master_key_v),
                (master_value, master_value_v),
                (first_key_in, first_key),
                (second_key_in, second_key),
                (first_value_in, first_value),
                (second_value_in, second_value),
                (key_cot, key_v),
                (value_cot, value_v),
                (normed, normed_v),
            )
        )
    ]
    barrier = pltpu.get_barrier_semaphore()
    for k in range(1, SIDE):
        pl.semaphore_signal(barrier, inc=1, device_id={"fs": along(0, k)}, device_id_type=MESH)
        pl.semaphore_signal(barrier, inc=1, device_id={"fs": along(1, k)}, device_id_type=MESH)
    for k in range(1, tp):
        pl.semaphore_signal(barrier, inc=1, device_id={"tp": lax.rem(my_tp + k, tp)}, device_id_type=MESH)

    for load in loads:
        load.start()

    for load in loads[2:8]:
        load.wait()
    master_all[z, y, :, :kc] = master_key_v[...].astype(BF16)
    master_all[z, y, :, kc:] = master_value_v[...].astype(BF16)
    moments[0, z, y, :, :kc] = first_key[...].astype(BF16)
    moments[0, z, y, :, kc:] = first_value[...].astype(BF16)
    moments[1, z, y, :, :kc] = second_key[...].astype(BF16)
    moments[1, z, y, :, kc:] = second_value[...].astype(BF16)
    loads[0].wait()
    loads[1].wait()

    pl.semaphore_wait(barrier, 2 * (SIDE - 1) + tp - 1)

    def by_core(body):
        for part in range(2):
            pl.when(core == part)(functools.partial(body, part))

    def line_at(part, k):
        if part == 0:
            return lax.rem(z + k, SIDE), y
        return z, lax.rem(y + k, SIDE)

    def group_at(part, k, cut=slice(None)):
        if part == 0:
            return cut, lax.rem(y + k, SIDE)
        return lax.rem(z + k, SIDE), cut

    def pack_arrays(at):
        return (0, moments.at[(slice(None), *at)]), (1, master_all.at[at])

    def basis_first(part):
        own = basis_all.at[core, z, y]
        for k in FAR:
            send(own, own, basis_send.at[0], basis_one.at[k], fs=along(part, k))
        for k in FAR:
            for a, block in pack_arrays((z, y)):
                send(block, block, pack_send.at[0, a], pack_one.at[a, k], fs=along(part, k))
        for j in (0,) + NEAR:
            block = basis_all.at[(core, *line_at(part, SIDE - j))]
            if j:
                wait_recv(block, basis_one.at[j])
            for k in FAR:
                send(block, block, basis_send.at[1], basis_two.at[k], fs=along(1 - part, k))
            if j:
                send(block, block, core_send.at[0], core_one.at[j], tp=partner)
        pack_first(part)

    def basis_second(part):
        for k in NEAR:
            group = basis_all.at[(core, *group_at(part, SIDE - k))]
            wait_recv(group, basis_two.at[k])
            send(group, group, core_send.at[1], core_two.at[k], tp=partner)
        for k in NEAR:
            wait_recv(basis_all.at[(1 - core, *line_at(1 - part, SIDE - k))], core_one.at[k])
            wait_recv(basis_all.at[(1 - core, *group_at(1 - part, SIDE - k))], core_two.at[k])

    def pack_first(part):
        for k in NEAR:
            for a, block in pack_arrays(line_at(part, SIDE - k)):
                wait_recv(block, pack_one.at[a, k])
        for k in (1, 7):
            for a, group in pack_arrays(group_at(part, 0)):
                send(group, group, pack_send.at[1, a], pack_near.at[a, k], fs=along(1 - part, k))

    def pack_step(k, part):
        ahead = 1 if k < SIDE // 2 else SIDE - 1
        for a, group in pack_arrays(group_at(part, SIDE - k)):
            wait_recv(group, pack_near.at[a, k])
            send(group, group, pack_send.at[2, a], pack_near.at[a, (k + ahead) % SIDE], fs=along(1 - part, ahead))
        if distance(k) == 2:
            cut = pl.ds(0, SIDE // 2) if k == 2 else pl.ds(SIDE // 2, SIDE // 2)
            for a, group in pack_arrays(group_at(part, SIDE - k, cut)):
                send(
                    group,
                    group,
                    pack_send.at[3, a],
                    pack_near.at[a, 0 if k == 2 else 4],
                    fs=along(1 - part, k),
                )

    def pack_pair(k, part):
        pack_step(k, part)
        pack_step(SIDE - k, part)

    def pack_last(a, part):
        for k in (3, 5):
            wait_recv(pack_arrays(group_at(part, SIDE - k))[a][1], pack_near.at[a, k])
        for slot, cut in ((0, pl.ds(0, SIDE // 2)), (4, pl.ds(SIDE // 2, SIDE // 2))):
            wait_recv(pack_arrays(group_at(part, SIDE // 2, cut))[a][1], pack_near.at[a, slot])

    by_core(basis_first)

    loads[8].wait()
    loads[9].wait()
    cot_t[:kc, :] = key_v[...].T
    cot_t[kc:, :] = value_v[...].T
    loads[10].wait()
    tile = 256

    @pl.loop(0, normed_v.shape[1] // tile)
    def _(t):
        at = pl.ds(pl.multiple_of(t * tile, tile), tile)
        grad_t[:, at] = jnp.dot(cot_t[...], normed_v[:, at], preferred_element_type=F32).astype(BF16)

    by_core(basis_second)

    depth = n * rows
    whole = jnp.concatenate(
        [basis_all[0].reshape(depth, 128), basis_all[1].reshape(depth, 128)], axis=1
    )
    sums = jnp.dot(grad_t[...], whole, preferred_element_type=F32).T.astype(BF16)
    rank_rows = first_key.shape[0]
    for j in range(n):
        partial[j] = sums[j * rank_rows : (j + 1) * rank_rows, :]

    order = sorted(
        ((dz, dy) for dz in range(SIDE) for dy in range(SIDE) if dz or dy),
        key=lambda d: -distance(d[0]) - distance(d[1]),
    )

    def device(dz, dy):
        return lax.rem(z + dz, SIDE) * SIDE + lax.rem(y + dy, SIDE)

    for dz, dy in order:
        target = device(dz, dy)
        send(partial.at[target], received.at[dz * SIDE + dy], part_send.at[0], part_recv.at[0], fs=target)

    by_core(functools.partial(pack_pair, 1))

    wait_recv(received.at[pl.ds(1, n - 1)], part_recv.at[0])
    low = partial[me].astype(F32)
    for k in range(1, n):
        low = low + received[k].astype(F32)

    chip_own[...] = jnp.full(chip_own.shape, jnp.sum(low * low), F32)
    low_own[...] = low.astype(BF16)
    low_all[me] = low.astype(BF16)
    for k in range(1, tp):
        send(chip_own, chip_all.at[k], chip_send.at[0], chip_recv.at[0], tp=lax.rem(my_tp + k, tp))
    for dz, dy in order:
        send(low_own, low_all.at[me], low_send.at[0], low_recv.at[0], fs=device(dz, dy))
    wait_recv(chip_all.at[pl.ds(1, tp - 1)], chip_recv.at[0])
    square = chip_own[...] + jnp.sum(chip_all[1:], axis=0)
    square_own[...] = square
    for dz, dy in order:
        send(square_own, square_all.at[dz * SIDE + dy], square_send.at[0], square_recv.at[0], fs=device(dz, dy))

    by_core(functools.partial(pack_pair, 2))

    wait_recv(square_all.at[pl.ds(1, n - 1)], square_recv.at[0])
    total = square_own[...] + jnp.sum(square_all[1:], axis=0)
    grad_scale = (1.0 / jnp.sqrt(total / count + norm_eps))[0:1, 0:1]
    scaled_out[...] = low * grad_scale

    by_core(functools.partial(pack_last, 0))
    wait_recv(low_all.at[pl.ds(0, n - 1)], low_recv.at[0])

    for j in range(n):
        scaled = low_all[j].astype(F32) * grad_scale
        moved = beta_first * moments[0, j // SIDE, j % SIDE].astype(F32) + (1.0 - beta_first) * scaled
        spread = beta_second * moments[1, j // SIDE, j % SIDE].astype(F32) + (1.0 - beta_second) * scaled * scaled
        turned[j * rank_rows : (j + 1) * rank_rows, :] = moved / (jnp.sqrt(spread) + epsilon)
    dirs[...] = turned[...].astype(BF16)

    by_core(functools.partial(pack_last, 1))

    blocks = pl.ds(0, SIDE - 1)
    wait_send(basis_all.at[0, blocks, 0], basis_send.at[0])
    wait_send(basis_all.at[0, blocks, 0], core_send.at[0])
    wait_send(basis_all.at[0, :, blocks], basis_send.at[1])
    wait_send(basis_all.at[0, :, blocks], core_send.at[1])
    for i, at in enumerate(((blocks, 0), (slice(None), pl.ds(0, 2)), (slice(None), pl.ds(0, 4)), (slice(None), 0))):
        for a, array in pack_arrays(at):
            wait_send(array, pack_send.at[i, a])
    wait_send(partial.at[pl.ds(0, n - 1)], part_send.at[0])
    wait_send(low_all.at[pl.ds(0, n - 1)], low_send.at[0])
    wait_send(chip_all.at[pl.ds(1, tp - 1)], chip_send.at[0])
    wait_send(square_all.at[pl.ds(1, n - 1)], square_send.at[0])


def final_kernel(
    basis_all,
    master_all,
    dirs,
    basis,
    master_key,
    master_value,
    scaled,
    first_key,
    second_key,
    first_value,
    second_value,
    copy_key,
    copy_value,
    step_key,
    step_value,
    new_key,
    new_value,
    new_first_key,
    new_second_key,
    new_first_value,
    new_second_value,
):
    kc = copy_key.shape[1]
    depth = copy_key.shape[0]
    block = depth // SIDE
    for i in range(SIDE):
        at = slice(i * block, (i + 1) * block)
        whole = jnp.concatenate([basis_all[h, i].reshape(block, 128) for h in range(2)], axis=1)
        held = master_all[i].reshape(block, dirs.shape[1])
        for cut, out in ((slice(0, kc), copy_key), (slice(kc, None), copy_value)):
            step = jnp.dot(whole, dirs[:, cut], preferred_element_type=F32)
            out[at, :] = (held[:, cut].astype(F32) - learn_rate * step).astype(BF16)

    for cut, master, step_out, new in (
        (slice(0, kc), master_key, step_key, new_key),
        (slice(kc, None), master_value, step_value, new_value),
    ):
        step = jnp.dot(basis[...], dirs[:, cut], preferred_element_type=F32)
        step_out[...] = step
        new[...] = master[...] - learn_rate * step
    for cut, first, second, new_first, new_second in (
        (slice(0, kc), first_key, second_key, new_first_key, new_second_key),
        (slice(kc, None), first_value, second_value, new_first_value, new_second_value),
    ):
        own = scaled[:, cut]
        new_first[...] = beta_first * first[...] + (1.0 - beta_first) * own
        new_second[...] = beta_second * second[...] + (1.0 - beta_second) * own * own


def on_device(
    n,
    tp,
    normed,
    key_cot,
    value_cot,
    basis,
    master_key,
    master_value,
    first_key,
    second_key,
    first_value,
    second_value,
):
    rows, rank = basis.shape
    d = rows * n
    kc, vc = key_cot.shape[1], value_cot.shape[1]
    cols = kc + vc
    tokens = normed.shape[0]
    rank_rows = first_key.shape[0]
    vmem = pl.BlockSpec(memory_space=pltpu.VMEM)
    hbm = pl.BlockSpec(memory_space=pltpu.HBM)
    dma = pltpu.SemaphoreType.DMA
    small = (1, 128)
    basis_all, master_all, dirs, scaled = pl.pallas_call(
        functools.partial(exchange_kernel, n, tp, rank * cols * tp),
        out_shape=(
            pltpu.VMEM((2, SIDE, SIDE, rows, rank // 2), BF16),
            pltpu.VMEM((SIDE, SIDE, rows, cols), BF16),
            pltpu.VMEM((rank, cols), BF16),
            pltpu.VMEM((rank_rows, cols), F32),
        ),
        in_specs=[hbm] * 10,
        out_specs=[vmem] * 4,
        scratch_shapes=[
            pltpu.VMEM(normed.shape, BF16),
            pltpu.VMEM(key_cot.shape, BF16),
            pltpu.VMEM(value_cot.shape, BF16),
            pltpu.VMEM(master_key.shape, F32),
            pltpu.VMEM(master_value.shape, F32),
            pltpu.VMEM(first_key.shape, F32),
            pltpu.VMEM(first_key.shape, F32),
            pltpu.VMEM(first_value.shape, F32),
            pltpu.VMEM(first_value.shape, F32),
            pltpu.VMEM((2, SIDE, SIDE, rank_rows, cols), BF16),
            pltpu.VMEM((cols, tokens), BF16),
            pltpu.VMEM((cols, d), BF16),
            pltpu.VMEM((n, rank_rows, cols), BF16),
            pltpu.VMEM((n, rank_rows, cols), BF16),
            pltpu.VMEM((rank_rows, cols), BF16),
            pltpu.VMEM((n, rank_rows, cols), BF16),
            pltpu.VMEM((rank, cols), F32),
            pltpu.VMEM(small, F32),
            pltpu.VMEM((tp, *small), F32),
            pltpu.VMEM(small, F32),
            pltpu.VMEM((n, *small), F32),
            dma((11,)),
            dma((2,)),
            dma((SIDE,)),
            dma((SIDE,)),
            dma((2,)),
            dma((SIDE,)),
            dma((SIDE,)),
            dma((4, 2)),
            dma((2, SIDE)),
            dma((2, SIDE)),
        ]
        + [dma((1,))] * 8,
        compiler_params=pltpu.CompilerParams(
            collective_id=0, has_side_effects=True, vmem_limit_bytes=62_914_560
        ),
    )(normed, key_cot, value_cot, basis, master_key, master_value, first_key, second_key, first_value, second_value)
    copy_key, copy_value, step_key, step_value, new_key, new_value, nfk, nsk, nfv, nsv = pl.pallas_call(
        final_kernel,
        out_shape=(
            jax.ShapeDtypeStruct((d, kc), BF16),
            jax.ShapeDtypeStruct((d, vc), BF16),
            jax.ShapeDtypeStruct((rows, kc), F32),
            jax.ShapeDtypeStruct((rows, vc), F32),
            jax.ShapeDtypeStruct((rows, kc), F32),
            jax.ShapeDtypeStruct((rows, vc), F32),
            jax.ShapeDtypeStruct(first_key.shape, F32),
            jax.ShapeDtypeStruct(first_key.shape, F32),
            jax.ShapeDtypeStruct(first_value.shape, F32),
            jax.ShapeDtypeStruct(first_value.shape, F32),
        ),
        in_specs=[vmem] * 11,
        out_specs=[vmem] * 10,
        compiler_params=pltpu.CompilerParams(vmem_limit_bytes=24 << 20),
    )(
        basis_all, master_all, dirs, basis, master_key, master_value, scaled, first_key, second_key, first_value, second_value
    )
    return (step_key, step_value, new_key, new_value, copy_key, copy_value, nfk, nsk, nfv, nsv)


def solution(mesh):
    split = P("fs", "tp")
    lone = P("fs", None)
    return jax.shard_map(
        functools.partial(on_device, mesh.shape["fs"], mesh.shape["tp"]),
        mesh=mesh,
        in_specs=(lone, split, split, lone) + (split,) * 6,
        out_specs=(split,) * 4 + (P(None, "tp"),) * 2 + (split,) * 4,
        check_vma=False,
    )
```

```python
import functools

import jax
import jax.numpy as jnp
from jax import lax
from jax.experimental import pallas as pl
from jax.experimental.pallas import tpu as pltpu
from jax.sharding import PartitionSpec as P

learn_rate = 0.05
beta_first = 0.9
beta_second = 0.9
epsilon = 1e-08
norm_eps = 1e-06

MESH = pl.DeviceIdType.MESH
F32 = jnp.float32
BF16 = jnp.bfloat16
SIDE = 8
NEAR = (1, 7, 2, 6, 3, 5, 4)
FAR = (4, 3, 5, 2, 6, 1, 7)


def distance(k):
    return min(k, SIDE - k)


def wait_recv(ref, sem):
    pltpu.make_async_remote_copy(
        src_ref=ref, dst_ref=ref, send_sem=sem, recv_sem=sem, device_id={"fs": 0}, device_id_type=MESH
    ).wait_recv()


def wait_send(ref, sem):
    pltpu.make_async_remote_copy(
        src_ref=ref, dst_ref=ref, send_sem=sem, recv_sem=sem, device_id={"fs": 0}, device_id_type=MESH
    ).wait_send()


def send(ref, target_ref, send_sem, recv_sem, **device):
    pltpu.make_async_remote_copy(
        src_ref=ref,
        dst_ref=target_ref,
        send_sem=send_sem,
        recv_sem=recv_sem,
        device_id=device,
        device_id_type=MESH,
    ).start()


def exchange_kernel(
    n,
    tp,
    count,
    normed,
    key_cot,
    value_cot,
    basis_in,
    master_key,
    master_value,
    first_key_in,
    second_key_in,
    first_value_in,
    second_value_in,
    basis_all,
    master_all,
    dirs,
    scaled_out,
    normed_v,
    key_v,
    value_v,
    master_key_v,
    master_value_v,
    first_key,
    second_key,
    first_value,
    second_value,
    moments,
    cot_t,
    grad_t,
    partial,
    received,
    low_own,
    low_all,
    turned,
    chip_own,
    chip_all,
    square_own,
    square_all,
    load_sem,
    basis_send,
    basis_one,
    basis_two,
    core_send,
    core_one,
    core_two,
    pack_send,
    pack_one,
    pack_near,
    part_send,
    part_recv,
    low_send,
    low_recv,
    chip_send,
    chip_recv,
    square_send,
    square_recv,
):
    me = lax.axis_index("fs")
    my_tp = lax.axis_index("tp")
    z, y = me // SIDE, lax.rem(me, SIDE)
    core = lax.rem(my_tp, 2)
    partner = my_tp + 1 - 2 * core

    def along(part, k):
        if part == 0:
            return lax.rem(z + k, SIDE) * SIDE + y
        return z * SIDE + lax.rem(y + k, SIDE)

    rows = basis_in.shape[0]
    kc = key_cot.shape[1]

    loads = [
        pltpu.make_async_copy(source, target, load_sem.at[i])
        for i, (source, target) in enumerate(
            (
                (basis_in.at[:, 0:128], basis_all.at[0, z, y]),
                (basis_in.at[:, 128:256], basis_all.at[1, z, y]),
                (master_key, master_key_v),
                (master_value, master_value_v),
                (first_key_in, first_key),
                (second_key_in, second_key),
                (first_value_in, first_value),
                (second_value_in, second_value),
                (key_cot, key_v),
                (value_cot, value_v),
                (normed, normed_v),
            )
        )
    ]
    barrier = pltpu.get_barrier_semaphore()
    for k in range(1, SIDE):
        pl.semaphore_signal(barrier, inc=1, device_id={"fs": along(0, k)}, device_id_type=MESH)
        pl.semaphore_signal(barrier, inc=1, device_id={"fs": along(1, k)}, device_id_type=MESH)
    for k in range(1, tp):
        pl.semaphore_signal(barrier, inc=1, device_id={"tp": lax.rem(my_tp + k, tp)}, device_id_type=MESH)

    for load in loads:
        load.start()

    for load in loads[2:8]:
        load.wait()
    master_all[z, y, :, :kc] = master_key_v[...].astype(BF16)
    master_all[z, y, :, kc:] = master_value_v[...].astype(BF16)
    moments[0, z, y, :, :kc] = first_key[...].astype(BF16)
    moments[0, z, y, :, kc:] = first_value[...].astype(BF16)
    moments[1, z, y, :, :kc] = second_key[...].astype(BF16)
    moments[1, z, y, :, kc:] = second_value[...].astype(BF16)
    loads[0].wait()
    loads[1].wait()

    pl.semaphore_wait(barrier, 2 * (SIDE - 1) + tp - 1)

    def by_core(body):
        for part in range(2):
            pl.when(core == part)(functools.partial(body, part))

    def line_at(part, k):
        if part == 0:
            return lax.rem(z + k, SIDE), y
        return z, lax.rem(y + k, SIDE)

    def group_at(part, k, cut=slice(None)):
        if part == 0:
            return cut, lax.rem(y + k, SIDE)
        return lax.rem(z + k, SIDE), cut

    def pack_arrays(at):
        return (0, moments.at[(slice(None), *at)]), (1, master_all.at[at])

    def basis_first(part):
        own = basis_all.at[core, z, y]
        for k in FAR:
            send(own, own, basis_send.at[0], basis_one.at[k], fs=along(part, k))
        for k in FAR:
            for a, block in pack_arrays((z, y)):
                send(block, block, pack_send.at[0, a], pack_one.at[a, k], fs=along(part, k))
        for j in (0,) + NEAR:
            block = basis_all.at[(core, *line_at(part, SIDE - j))]
            if j:
                wait_recv(block, basis_one.at[j])
            for k in FAR:
                send(block, block, basis_send.at[1], basis_two.at[k], fs=along(1 - part, k))
            if j:
                send(block, block, core_send.at[0], core_one.at[j], tp=partner)
        pack_first(part)

    def basis_second(part):
        for k in NEAR:
            group = basis_all.at[(core, *group_at(part, SIDE - k))]
            wait_recv(group, basis_two.at[k])
            send(group, group, core_send.at[1], core_two.at[k], tp=partner)
        for k in NEAR:
            wait_recv(basis_all.at[(1 - core, *line_at(1 - part, SIDE - k))], core_one.at[k])
            wait_recv(basis_all.at[(1 - core, *group_at(1 - part, SIDE - k))], core_two.at[k])

    def pack_first(part):
        for k in NEAR:
            for a, block in pack_arrays(line_at(part, SIDE - k)):
                wait_recv(block, pack_one.at[a, k])
        for k in (1, 7):
            for a, group in pack_arrays(group_at(part, 0)):
                send(group, group, pack_send.at[1, a], pack_near.at[a, k], fs=along(1 - part, k))

    def pack_step(k, part):
        ahead = 1 if k < SIDE // 2 else SIDE - 1
        for a, group in pack_arrays(group_at(part, SIDE - k)):
            wait_recv(group, pack_near.at[a, k])
            send(group, group, pack_send.at[2, a], pack_near.at[a, (k + ahead) % SIDE], fs=along(1 - part, ahead))

    def pack_far(part):
        for k, ahead, slot, start in ((3, 1, 0, 0), (5, 7, 4, SIDE // 2)):
            for a, group in pack_arrays(group_at(part, SIDE - k)):
                wait_recv(group, pack_near.at[a, k])
            for a, group in pack_arrays(group_at(part, SIDE - k, pl.ds(start, SIDE // 2))):
                send(group, group, pack_send.at[3, a], pack_near.at[a, slot], fs=along(1 - part, ahead))

    def pack_pair(k, part):
        pack_step(k, part)
        pack_step(SIDE - k, part)

    def pack_last(a, part):
        for slot, cut in ((0, pl.ds(0, SIDE // 2)), (4, pl.ds(SIDE // 2, SIDE // 2))):
            wait_recv(pack_arrays(group_at(part, SIDE // 2, cut))[a][1], pack_near.at[a, slot])

    by_core(basis_first)

    loads[8].wait()
    loads[9].wait()
    cot_t[:kc, :] = key_v[...].T
    cot_t[kc:, :] = value_v[...].T
    loads[10].wait()
    tile = 256

    @pl.loop(0, normed_v.shape[1] // tile)
    def _(t):
        at = pl.ds(pl.multiple_of(t * tile, tile), tile)
        grad_t[:, at] = jnp.dot(cot_t[...], normed_v[:, at], preferred_element_type=F32).astype(BF16)

    by_core(basis_second)

    depth = n * rows
    whole = jnp.concatenate(
        [basis_all[0].reshape(depth, 128), basis_all[1].reshape(depth, 128)], axis=1
    )
    sums = jnp.dot(grad_t[...], whole, preferred_element_type=F32).T.astype(BF16)
    rank_rows = first_key.shape[0]
    for j in range(n):
        partial[j] = sums[j * rank_rows : (j + 1) * rank_rows, :]

    order = sorted(
        ((dz, dy) for dz in range(SIDE) for dy in range(SIDE) if dz or dy),
        key=lambda d: -distance(d[0]) - distance(d[1]),
    )

    def device(dz, dy):
        return lax.rem(z + dz, SIDE) * SIDE + lax.rem(y + dy, SIDE)

    for dz, dy in order:
        target = device(dz, dy)
        send(partial.at[target], received.at[dz * SIDE + dy], part_send.at[0], part_recv.at[0], fs=target)

    by_core(functools.partial(pack_pair, 1))

    wait_recv(received.at[pl.ds(1, n - 1)], part_recv.at[0])
    low = partial[me].astype(F32)
    for k in range(1, n):
        low = low + received[k].astype(F32)

    chip_own[...] = jnp.full(chip_own.shape, jnp.sum(low * low), F32)
    low_own[...] = low.astype(BF16)
    low_all[z, y] = low.astype(BF16)
    for k in range(1, tp):
        send(chip_own, chip_all.at[k], chip_send.at[0], chip_recv.at[0], tp=lax.rem(my_tp + k, tp))

    def low_first(part):
        for k in FAR:
            send(low_own, low_all.at[z, y], low_send.at[0], low_recv.at[0], fs=along(part, k))

    def low_second(part):
        line = low_all.at[pl.ds(0, SIDE - 1), 0]
        wait_recv(line, low_recv.at[0])
        group = low_all.at[group_at(part, 0)]
        for k in FAR:
            send(group, group, low_send.at[1], low_recv.at[1], fs=along(1 - part, k))

    by_core(low_first)
    by_core(functools.partial(pack_pair, 2))
    wait_recv(chip_all.at[pl.ds(1, tp - 1)], chip_recv.at[0])
    square = chip_own[...] + jnp.sum(chip_all[1:], axis=0)
    square_own[...] = square
    for dz, dy in order:
        send(square_own, square_all.at[dz * SIDE + dy], square_send.at[0], square_recv.at[0], fs=device(dz, dy))

    by_core(low_second)
    by_core(pack_far)

    wait_recv(square_all.at[pl.ds(1, n - 1)], square_recv.at[0])
    total = square_own[...] + jnp.sum(square_all[1:], axis=0)
    grad_scale = (1.0 / jnp.sqrt(total / count + norm_eps))[0:1, 0:1]
    scaled_out[...] = low * grad_scale

    by_core(functools.partial(pack_last, 0))
    wait_recv(low_all.at[:, pl.ds(0, SIDE - 1)], low_recv.at[1])

    for j in range(n):
        scaled = low_all[j // SIDE, j % SIDE].astype(F32) * grad_scale
        moved = beta_first * moments[0, j // SIDE, j % SIDE].astype(F32) + (1.0 - beta_first) * scaled
        spread = beta_second * moments[1, j // SIDE, j % SIDE].astype(F32) + (1.0 - beta_second) * scaled * scaled
        turned[j * rank_rows : (j + 1) * rank_rows, :] = moved / (jnp.sqrt(spread) + epsilon)
    dirs[...] = turned[...].astype(BF16)

    by_core(functools.partial(pack_last, 1))

    blocks = pl.ds(0, SIDE - 1)
    wait_send(basis_all.at[0, blocks, 0], basis_send.at[0])
    wait_send(basis_all.at[0, blocks, 0], core_send.at[0])
    wait_send(basis_all.at[0, :, blocks], basis_send.at[1])
    wait_send(basis_all.at[0, :, blocks], core_send.at[1])
    for i, at in enumerate(((blocks, 0), (slice(None), pl.ds(0, 2)), (slice(None), pl.ds(0, 4)), (slice(None), 0))):
        for a, array in pack_arrays(at):
            wait_send(array, pack_send.at[i, a])
    wait_send(partial.at[pl.ds(0, n - 1)], part_send.at[0])
    wait_send(low_all.at[blocks, 0], low_send.at[0])
    wait_send(low_all.at[:, blocks], low_send.at[1])
    wait_send(chip_all.at[pl.ds(1, tp - 1)], chip_send.at[0])
    wait_send(square_all.at[pl.ds(1, n - 1)], square_send.at[0])


def final_kernel(
    basis_all,
    master_all,
    dirs,
    basis,
    master_key,
    master_value,
    scaled,
    first_key,
    second_key,
    first_value,
    second_value,
    copy_key,
    copy_value,
    step_key,
    step_value,
    new_key,
    new_value,
    new_first_key,
    new_second_key,
    new_first_value,
    new_second_value,
):
    kc = copy_key.shape[1]
    depth = copy_key.shape[0]
    block = depth // SIDE
    for i in range(SIDE):
        at = slice(i * block, (i + 1) * block)
        whole = jnp.concatenate([basis_all[h, i].reshape(block, 128) for h in range(2)], axis=1)
        held = master_all[i].reshape(block, dirs.shape[1])
        for cut, out in ((slice(0, kc), copy_key), (slice(kc, None), copy_value)):
            step = jnp.dot(whole, dirs[:, cut], preferred_element_type=F32)
            out[at, :] = (held[:, cut].astype(F32) - learn_rate * step).astype(BF16)

    for cut, master, step_out, new in (
        (slice(0, kc), master_key, step_key, new_key),
        (slice(kc, None), master_value, step_value, new_value),
    ):
        step = jnp.dot(basis[...], dirs[:, cut], preferred_element_type=F32)
        step_out[...] = step
        new[...] = master[...] - learn_rate * step
    for cut, first, second, new_first, new_second in (
        (slice(0, kc), first_key, second_key, new_first_key, new_second_key),
        (slice(kc, None), first_value, second_value, new_first_value, new_second_value),
    ):
        own = scaled[:, cut]
        new_first[...] = beta_first * first[...] + (1.0 - beta_first) * own
        new_second[...] = beta_second * second[...] + (1.0 - beta_second) * own * own


def on_device(
    n,
    tp,
    normed,
    key_cot,
    value_cot,
    basis,
    master_key,
    master_value,
    first_key,
    second_key,
    first_value,
    second_value,
):
    rows, rank = basis.shape
    d = rows * n
    kc, vc = key_cot.shape[1], value_cot.shape[1]
    cols = kc + vc
    tokens = normed.shape[0]
    rank_rows = first_key.shape[0]
    vmem = pl.BlockSpec(memory_space=pltpu.VMEM)
    hbm = pl.BlockSpec(memory_space=pltpu.HBM)
    dma = pltpu.SemaphoreType.DMA
    small = (1, 128)
    basis_all, master_all, dirs, scaled = pl.pallas_call(
        functools.partial(exchange_kernel, n, tp, rank * cols * tp),
        out_shape=(
            pltpu.VMEM((2, SIDE, SIDE, rows, rank // 2), BF16),
            pltpu.VMEM((SIDE, SIDE, rows, cols), BF16),
            pltpu.VMEM((rank, cols), BF16),
            pltpu.VMEM((rank_rows, cols), F32),
        ),
        in_specs=[hbm] * 10,
        out_specs=[vmem] * 4,
        scratch_shapes=[
            pltpu.VMEM(normed.shape, BF16),
            pltpu.VMEM(key_cot.shape, BF16),
            pltpu.VMEM(value_cot.shape, BF16),
            pltpu.VMEM(master_key.shape, F32),
            pltpu.VMEM(master_value.shape, F32),
            pltpu.VMEM(first_key.shape, F32),
            pltpu.VMEM(first_key.shape, F32),
            pltpu.VMEM(first_value.shape, F32),
            pltpu.VMEM(first_value.shape, F32),
            pltpu.VMEM((2, SIDE, SIDE, rank_rows, cols), BF16),
            pltpu.VMEM((cols, tokens), BF16),
            pltpu.VMEM((cols, d), BF16),
            pltpu.VMEM((n, rank_rows, cols), BF16),
            pltpu.VMEM((n, rank_rows, cols), BF16),
            pltpu.VMEM((rank_rows, cols), BF16),
            pltpu.VMEM((SIDE, SIDE, rank_rows, cols), BF16),
            pltpu.VMEM((rank, cols), F32),
            pltpu.VMEM(small, F32),
            pltpu.VMEM((tp, *small), F32),
            pltpu.VMEM(small, F32),
            pltpu.VMEM((n, *small), F32),
            dma((11,)),
            dma((2,)),
            dma((SIDE,)),
            dma((SIDE,)),
            dma((2,)),
            dma((SIDE,)),
            dma((SIDE,)),
            dma((4, 2)),
            dma((2, SIDE)),
            dma((2, SIDE)),
        ]
        + [dma((2,))] * 8,
        compiler_params=pltpu.CompilerParams(
            collective_id=0, has_side_effects=True, vmem_limit_bytes=62_914_560
        ),
    )(normed, key_cot, value_cot, basis, master_key, master_value, first_key, second_key, first_value, second_value)
    copy_key, copy_value, step_key, step_value, new_key, new_value, nfk, nsk, nfv, nsv = pl.pallas_call(
        final_kernel,
        out_shape=(
            jax.ShapeDtypeStruct((d, kc), BF16),
            jax.ShapeDtypeStruct((d, vc), BF16),
            jax.ShapeDtypeStruct((rows, kc), F32),
            jax.ShapeDtypeStruct((rows, vc), F32),
            jax.ShapeDtypeStruct((rows, kc), F32),
            jax.ShapeDtypeStruct((rows, vc), F32),
            jax.ShapeDtypeStruct(first_key.shape, F32),
            jax.ShapeDtypeStruct(first_key.shape, F32),
            jax.ShapeDtypeStruct(first_value.shape, F32),
            jax.ShapeDtypeStruct(first_value.shape, F32),
        ),
        in_specs=[vmem] * 11,
        out_specs=[vmem] * 10,
        compiler_params=pltpu.CompilerParams(vmem_limit_bytes=24 << 20),
    )(
        basis_all, master_all, dirs, basis, master_key, master_value, scaled, first_key, second_key, first_value, second_value
    )
    return (step_key, step_value, new_key, new_value, copy_key, copy_value, nfk, nsk, nfv, nsv)


def solution(mesh):
    split = P("fs", "tp")
    lone = P("fs", None)
    return jax.shard_map(
        functools.partial(on_device, mesh.shape["fs"], mesh.shape["tp"]),
        mesh=mesh,
        in_specs=(lone, split, split, lone) + (split,) * 6,
        out_specs=(split,) * 4 + (P(None, "tp"),) * 2 + (split,) * 4,
        check_vma=False,
    )
```

```python
import functools

import jax
import jax.numpy as jnp
from jax import lax
from jax.experimental import pallas as pl
from jax.experimental.pallas import tpu as pltpu
from jax.sharding import PartitionSpec as P

learn_rate = 0.05
beta_first = 0.9
beta_second = 0.9
epsilon = 1e-08
norm_eps = 1e-06

MESH = pl.DeviceIdType.MESH
F32 = jnp.float32
BF16 = jnp.bfloat16
SIDE = 8
NEAR = (1, 7, 2, 6, 3, 5, 4)
FAR = (4, 3, 5, 2, 6, 1, 7)


def distance(k):
    return min(k, SIDE - k)


def wait_recv(ref, sem):
    pltpu.make_async_remote_copy(
        src_ref=ref, dst_ref=ref, send_sem=sem, recv_sem=sem, device_id={"fs": 0}, device_id_type=MESH
    ).wait_recv()


def wait_send(ref, sem):
    pltpu.make_async_remote_copy(
        src_ref=ref, dst_ref=ref, send_sem=sem, recv_sem=sem, device_id={"fs": 0}, device_id_type=MESH
    ).wait_send()


def send(ref, target_ref, send_sem, recv_sem, **device):
    pltpu.make_async_remote_copy(
        src_ref=ref,
        dst_ref=target_ref,
        send_sem=send_sem,
        recv_sem=recv_sem,
        device_id=device,
        device_id_type=MESH,
    ).start()


def exchange_kernel(
    n,
    tp,
    count,
    normed,
    key_cot,
    value_cot,
    basis_in,
    master_key,
    master_value,
    first_key_in,
    second_key_in,
    first_value_in,
    second_value_in,
    basis_all,
    master_all,
    dirs,
    scaled_out,
    normed_v,
    key_v,
    value_v,
    master_key_v,
    master_value_v,
    first_key,
    second_key,
    first_value,
    second_value,
    moments,
    cot_t,
    grad_t,
    partial,
    received,
    low_own,
    low_all,
    low_part,
    square_part,
    first_part,
    second_part,
    chip_own,
    chip_all,
    square_own,
    square_all,
    load_sem,
    basis_send,
    basis_one,
    basis_two,
    core_send,
    core_one,
    core_two,
    pack_send,
    pack_one,
    pack_near,
    part_send,
    part_recv,
    low_send,
    low_recv,
    chip_send,
    chip_recv,
    square_send,
    square_recv,
):
    me = lax.axis_index("fs")
    my_tp = lax.axis_index("tp")
    z, y = me // SIDE, lax.rem(me, SIDE)
    core = lax.rem(my_tp, 2)
    partner = my_tp + 1 - 2 * core

    def along(part, k):
        if part == 0:
            return lax.rem(z + k, SIDE) * SIDE + y
        return z * SIDE + lax.rem(y + k, SIDE)

    rows = basis_in.shape[0]
    kc = key_cot.shape[1]

    loads = [
        pltpu.make_async_copy(source, target, load_sem.at[i])
        for i, (source, target) in enumerate(
            (
                (basis_in.at[:, 0:128], basis_all.at[0, z, y]),
                (basis_in.at[:, 128:256], basis_all.at[1, z, y]),
                (master_key, master_key_v),
                (master_value, master_value_v),
                (first_key_in, first_key),
                (second_key_in, second_key),
                (first_value_in, first_value),
                (second_value_in, second_value),
                (key_cot, key_v),
                (value_cot, value_v),
                (normed, normed_v),
            )
        )
    ]
    barrier = pltpu.get_barrier_semaphore()
    for k in range(1, SIDE):
        pl.semaphore_signal(barrier, inc=1, device_id={"fs": along(0, k)}, device_id_type=MESH)
        pl.semaphore_signal(barrier, inc=1, device_id={"fs": along(1, k)}, device_id_type=MESH)
    for k in range(1, tp):
        pl.semaphore_signal(barrier, inc=1, device_id={"tp": lax.rem(my_tp + k, tp)}, device_id_type=MESH)

    for load in loads:
        load.start()

    loads[0].wait()
    loads[1].wait()

    pl.semaphore_wait(barrier, 2 * (SIDE - 1) + tp - 1)

    def by_core(body):
        for part in range(2):
            pl.when(core == part)(functools.partial(body, part))

    def line_at(part, k):
        if part == 0:
            return lax.rem(z + k, SIDE), y
        return z, lax.rem(y + k, SIDE)

    def group_at(part, k, cut=slice(None)):
        if part == 0:
            return cut, lax.rem(y + k, SIDE)
        return lax.rem(z + k, SIDE), cut

    def pack_arrays(at):
        return (0, moments.at[(slice(None), *at)]), (1, master_all.at[at])

    def basis_first(part):
        own = basis_all.at[core, z, y]
        for k in FAR:
            send(own, own, basis_send.at[0], basis_one.at[k], fs=along(part, k))
        for load in loads[2:8]:
            load.wait()
        master_all[z, y, :, :kc] = master_key_v[...].astype(BF16)
        master_all[z, y, :, kc:] = master_value_v[...].astype(BF16)
        moments[0, z, y, :, :kc] = first_key[...].astype(BF16)
        moments[0, z, y, :, kc:] = first_value[...].astype(BF16)
        moments[1, z, y, :, :kc] = second_key[...].astype(BF16)
        moments[1, z, y, :, kc:] = second_value[...].astype(BF16)
        for k in FAR:
            for a, block in pack_arrays((z, y)):
                send(block, block, pack_send.at[0, a], pack_one.at[a, k], fs=along(part, k))
        for j in (0,) + NEAR:
            block = basis_all.at[(core, *line_at(part, SIDE - j))]
            if j:
                wait_recv(block, basis_one.at[j])
            for k in FAR:
                send(block, block, basis_send.at[1], basis_two.at[k], fs=along(1 - part, k))
            if j:
                send(block, block, core_send.at[0], core_one.at[j], tp=partner)
        pack_first(part)

    def basis_second(part):
        for k in NEAR:
            group = basis_all.at[(core, *group_at(part, SIDE - k))]
            wait_recv(group, basis_two.at[k])
            send(group, group, core_send.at[1], core_two.at[k], tp=partner)
        for k in NEAR:
            wait_recv(basis_all.at[(1 - core, *line_at(1 - part, SIDE - k))], core_one.at[k])
            wait_recv(basis_all.at[(1 - core, *group_at(1 - part, SIDE - k))], core_two.at[k])

    def pack_first(part):
        for k in NEAR:
            for a, block in pack_arrays(line_at(part, SIDE - k)):
                wait_recv(block, pack_one.at[a, k])
        for k in (1, 7):
            for a, group in pack_arrays(group_at(part, 0)):
                send(group, group, pack_send.at[1, a], pack_near.at[a, k], fs=along(1 - part, k))

    def pack_step(k, part):
        ahead = 1 if k < SIDE // 2 else SIDE - 1
        for a, group in pack_arrays(group_at(part, SIDE - k)):
            wait_recv(group, pack_near.at[a, k])
            send(group, group, pack_send.at[2, a], pack_near.at[a, (k + ahead) % SIDE], fs=along(1 - part, ahead))

    def pack_far(part):
        for k, ahead, slot, start in ((3, 1, 0, 0), (5, 7, 4, SIDE // 2)):
            for a, group in pack_arrays(group_at(part, SIDE - k)):
                wait_recv(group, pack_near.at[a, k])
            for a, group in pack_arrays(group_at(part, SIDE - k, pl.ds(start, SIDE // 2))):
                send(group, group, pack_send.at[3, a], pack_near.at[a, slot], fs=along(1 - part, ahead))

    def pack_pair(k, part):
        pack_step(k, part)
        pack_step(SIDE - k, part)

    def pack_last(a, part):
        for slot, cut in ((0, pl.ds(0, SIDE // 2)), (4, pl.ds(SIDE // 2, SIDE // 2))):
            wait_recv(pack_arrays(group_at(part, SIDE // 2, cut))[a][1], pack_near.at[a, slot])

    by_core(basis_first)

    loads[8].wait()
    loads[9].wait()
    cot_t[:kc, :] = key_v[...].T
    cot_t[kc:, :] = value_v[...].T
    loads[10].wait()
    tile = 256

    @pl.loop(0, normed_v.shape[1] // tile)
    def _(t):
        at = pl.ds(pl.multiple_of(t * tile, tile), tile)
        grad_t[:, at] = jnp.dot(cot_t[...], normed_v[:, at], preferred_element_type=F32).astype(BF16)

    by_core(basis_second)

    depth = n * rows
    whole = jnp.concatenate(
        [basis_all[0].reshape(depth, 128), basis_all[1].reshape(depth, 128)], axis=1
    )
    sums = jnp.dot(grad_t[...], whole, preferred_element_type=F32).T.astype(BF16)
    rank_rows = first_key.shape[0]
    for j in range(n):
        partial[j] = sums[j * rank_rows : (j + 1) * rank_rows, :]

    order = sorted(
        ((dz, dy) for dz in range(SIDE) for dy in range(SIDE) if dz or dy),
        key=lambda d: -distance(d[0]) - distance(d[1]),
    )

    def device(dz, dy):
        return lax.rem(z + dz, SIDE) * SIDE + lax.rem(y + dy, SIDE)

    for dz, dy in order:
        target = device(dz, dy)
        send(partial.at[target], received.at[dz * SIDE + dy], part_send.at[0], part_recv.at[0], fs=target)

    by_core(functools.partial(pack_pair, 1))

    wait_recv(received.at[pl.ds(1, n - 1)], part_recv.at[0])
    low = partial[me].astype(F32)
    for k in range(1, n):
        low = low + received[k].astype(F32)

    chip_own[...] = jnp.full(chip_own.shape, jnp.sum(low * low), F32)
    low_own[...] = low.astype(BF16)
    low_all[z, y] = low.astype(BF16)
    for k in range(1, tp):
        send(chip_own, chip_all.at[k], chip_send.at[0], chip_recv.at[0], tp=lax.rem(my_tp + k, tp))

    def low_first(part):
        for k in FAR:
            send(low_own, low_all.at[z, y], low_send.at[0], low_recv.at[0], fs=along(part, k))

    def low_second(part):
        line = low_all.at[pl.ds(0, SIDE - 1), 0]
        wait_recv(line, low_recv.at[0])
        group = low_all.at[group_at(part, 0)]
        for k in FAR:
            send(group, group, low_send.at[1], low_recv.at[1], fs=along(1 - part, k))

    by_core(low_first)
    by_core(functools.partial(pack_pair, 2))
    wait_recv(chip_all.at[pl.ds(1, tp - 1)], chip_recv.at[0])
    square = chip_own[...] + jnp.sum(chip_all[1:], axis=0)
    square_own[...] = square
    for dz, dy in order:
        send(square_own, square_all.at[dz * SIDE + dy], square_send.at[0], square_recv.at[0], fs=device(dz, dy))

    by_core(low_second)
    by_core(pack_far)

    wait_recv(low_all.at[:, pl.ds(0, SIDE - 1)], low_recv.at[1])
    for j in range(n):
        at = slice(j * rank_rows, (j + 1) * rank_rows)
        each = low_all[j // SIDE, j % SIDE].astype(F32)
        low_part[at, :] = (1.0 - beta_first) * each
        square_part[at, :] = (1.0 - beta_second) * each * each
    by_core(functools.partial(pack_last, 0))
    for j in range(n):
        at = slice(j * rank_rows, (j + 1) * rank_rows)
        first_part[at, :] = beta_first * moments[0, j // SIDE, j % SIDE].astype(F32)
        second_part[at, :] = beta_second * moments[1, j // SIDE, j % SIDE].astype(F32)

    wait_recv(square_all.at[pl.ds(1, n - 1)], square_recv.at[0])
    total = square_own[...] + jnp.sum(square_all[1:], axis=0)
    grad_scale = (1.0 / jnp.sqrt(total / count + norm_eps))[0:1, 0:1]
    scaled_out[...] = low * grad_scale
    height = n * rank_rows // SIDE
    for i in range(SIDE):
        at = slice(i * height, (i + 1) * height)
        moved = first_part[at, :] + grad_scale * low_part[at, :]
        spread = second_part[at, :] + grad_scale * grad_scale * square_part[at, :]
        dirs[at, :] = (moved / (jnp.sqrt(spread) + epsilon)).astype(BF16)

    by_core(functools.partial(pack_last, 1))

    blocks = pl.ds(0, SIDE - 1)
    wait_send(basis_all.at[0, blocks, 0], basis_send.at[0])
    wait_send(basis_all.at[0, blocks, 0], core_send.at[0])
    wait_send(basis_all.at[0, :, blocks], basis_send.at[1])
    wait_send(basis_all.at[0, :, blocks], core_send.at[1])
    for i, at in enumerate(((blocks, 0), (slice(None), pl.ds(0, 2)), (slice(None), pl.ds(0, 4)), (slice(None), 0))):
        for a, array in pack_arrays(at):
            wait_send(array, pack_send.at[i, a])
    wait_send(partial.at[pl.ds(0, n - 1)], part_send.at[0])
    wait_send(low_all.at[blocks, 0], low_send.at[0])
    wait_send(low_all.at[:, blocks], low_send.at[1])
    wait_send(chip_all.at[pl.ds(1, tp - 1)], chip_send.at[0])
    wait_send(square_all.at[pl.ds(1, n - 1)], square_send.at[0])


def final_kernel(
    basis_all,
    master_all,
    dirs,
    basis,
    master_key,
    master_value,
    scaled,
    first_key,
    second_key,
    first_value,
    second_value,
    copy_key,
    copy_value,
    step_key,
    step_value,
    new_key,
    new_value,
    new_first_key,
    new_second_key,
    new_first_value,
    new_second_value,
):
    kc = copy_key.shape[1]
    depth = copy_key.shape[0]
    block = depth // SIDE
    for i in range(SIDE):
        at = slice(i * block, (i + 1) * block)
        whole = jnp.concatenate([basis_all[h, i].reshape(block, 128) for h in range(2)], axis=1)
        held = master_all[i].reshape(block, dirs.shape[1])
        for cut, out in ((slice(0, kc), copy_key), (slice(kc, None), copy_value)):
            step = jnp.dot(whole, dirs[:, cut], preferred_element_type=F32)
            out[at, :] = (held[:, cut].astype(F32) - learn_rate * step).astype(BF16)

    for cut, master, step_out, new in (
        (slice(0, kc), master_key, step_key, new_key),
        (slice(kc, None), master_value, step_value, new_value),
    ):
        step = jnp.dot(basis[...], dirs[:, cut], preferred_element_type=F32)
        step_out[...] = step
        new[...] = master[...] - learn_rate * step
    for cut, first, second, new_first, new_second in (
        (slice(0, kc), first_key, second_key, new_first_key, new_second_key),
        (slice(kc, None), first_value, second_value, new_first_value, new_second_value),
    ):
        own = scaled[:, cut]
        new_first[...] = beta_first * first[...] + (1.0 - beta_first) * own
        new_second[...] = beta_second * second[...] + (1.0 - beta_second) * own * own


def on_device(
    n,
    tp,
    normed,
    key_cot,
    value_cot,
    basis,
    master_key,
    master_value,
    first_key,
    second_key,
    first_value,
    second_value,
):
    rows, rank = basis.shape
    d = rows * n
    kc, vc = key_cot.shape[1], value_cot.shape[1]
    cols = kc + vc
    tokens = normed.shape[0]
    rank_rows = first_key.shape[0]
    vmem = pl.BlockSpec(memory_space=pltpu.VMEM)
    hbm = pl.BlockSpec(memory_space=pltpu.HBM)
    dma = pltpu.SemaphoreType.DMA
    small = (1, 128)
    basis_all, master_all, dirs, scaled = pl.pallas_call(
        functools.partial(exchange_kernel, n, tp, rank * cols * tp),
        out_shape=(
            pltpu.VMEM((2, SIDE, SIDE, rows, rank // 2), BF16),
            pltpu.VMEM((SIDE, SIDE, rows, cols), BF16),
            pltpu.VMEM((rank, cols), BF16),
            pltpu.VMEM((rank_rows, cols), F32),
        ),
        in_specs=[hbm] * 10,
        out_specs=[vmem] * 4,
        scratch_shapes=[
            pltpu.VMEM(normed.shape, BF16),
            pltpu.VMEM(key_cot.shape, BF16),
            pltpu.VMEM(value_cot.shape, BF16),
            pltpu.VMEM(master_key.shape, F32),
            pltpu.VMEM(master_value.shape, F32),
            pltpu.VMEM(first_key.shape, F32),
            pltpu.VMEM(first_key.shape, F32),
            pltpu.VMEM(first_value.shape, F32),
            pltpu.VMEM(first_value.shape, F32),
            pltpu.VMEM((2, SIDE, SIDE, rank_rows, cols), BF16),
            pltpu.VMEM((cols, tokens), BF16),
            pltpu.VMEM((cols, d), BF16),
            pltpu.VMEM((n, rank_rows, cols), BF16),
            pltpu.VMEM((n, rank_rows, cols), BF16),
            pltpu.VMEM((rank_rows, cols), BF16),
            pltpu.VMEM((SIDE, SIDE, rank_rows, cols), BF16),
            pltpu.VMEM((rank, cols), F32),
            pltpu.VMEM((rank, cols), F32),
            pltpu.VMEM((rank, cols), F32),
            pltpu.VMEM((rank, cols), F32),
            pltpu.VMEM(small, F32),
            pltpu.VMEM((tp, *small), F32),
            pltpu.VMEM(small, F32),
            pltpu.VMEM((n, *small), F32),
            dma((11,)),
            dma((2,)),
            dma((SIDE,)),
            dma((SIDE,)),
            dma((2,)),
            dma((SIDE,)),
            dma((SIDE,)),
            dma((4, 2)),
            dma((2, SIDE)),
            dma((2, SIDE)),
        ]
        + [dma((2,))] * 8,
        compiler_params=pltpu.CompilerParams(
            collective_id=0, has_side_effects=True, vmem_limit_bytes=62_914_560
        ),
    )(normed, key_cot, value_cot, basis, master_key, master_value, first_key, second_key, first_value, second_value)
    copy_key, copy_value, step_key, step_value, new_key, new_value, nfk, nsk, nfv, nsv = pl.pallas_call(
        final_kernel,
        out_shape=(
            jax.ShapeDtypeStruct((d, kc), BF16),
            jax.ShapeDtypeStruct((d, vc), BF16),
            jax.ShapeDtypeStruct((rows, kc), F32),
            jax.ShapeDtypeStruct((rows, vc), F32),
            jax.ShapeDtypeStruct((rows, kc), F32),
            jax.ShapeDtypeStruct((rows, vc), F32),
            jax.ShapeDtypeStruct(first_key.shape, F32),
            jax.ShapeDtypeStruct(first_key.shape, F32),
            jax.ShapeDtypeStruct(first_value.shape, F32),
            jax.ShapeDtypeStruct(first_value.shape, F32),
        ),
        in_specs=[vmem] * 11,
        out_specs=[vmem] * 10,
        compiler_params=pltpu.CompilerParams(vmem_limit_bytes=24 << 20),
    )(
        basis_all, master_all, dirs, basis, master_key, master_value, scaled, first_key, second_key, first_value, second_value
    )
    return (step_key, step_value, new_key, new_value, copy_key, copy_value, nfk, nsk, nfv, nsv)


def solution(mesh):
    split = P("fs", "tp")
    lone = P("fs", None)
    return jax.shard_map(
        functools.partial(on_device, mesh.shape["fs"], mesh.shape["tp"]),
        mesh=mesh,
        in_specs=(lone, split, split, lone) + (split,) * 6,
        out_specs=(split,) * 4 + (P(None, "tp"),) * 2 + (split,) * 4,
        check_vma=False,
    )
```
